512 devices in a mesh: dp: 4 (over x), kv: 64 (over z, y), tp: 2 (over core).
Axes of the slice: x: 4, y: 8, z: 8, core: 2. Of those that a mesh axis runs over, the one named last changes fastest.
Arguments:
- tokens: bfloat16 [4, 24576, 2048], P('dp', 'kv'), may hold values from -21 to 21
- seq_lengths: int32 [4], P('dp'), may hold values from 1 to 24576, 36864 in all
- block_picks: int32 [4, 384, 4, 16], P('dp', 'kv', 'tp'), may hold values from -1 to 377, as said below
- w_query: bfloat16 [2048, 1024], P('kv', 'tp'), may hold values from -0.125 to 0.125
- w_key: bfloat16 [2048, 256], P('kv', 'tp'), may hold values from -0.125 to 0.125
- w_value: bfloat16 [2048, 256], P('kv', 'tp'), may hold values from -0.125 to 0.125
- w_gate: bfloat16 [2048, 32], replicated, may hold values from -0.125 to 0.125
- w_ckey: bfloat16 [4096, 64], replicated, may hold values from -0.09375 to 0.09375
- w_cvalue: bfloat16 [4096, 64], replicated, may hold values from -0.09375 to 0.09375
- w_out: bfloat16 [1024, 2048], P('tp', 'kv'), may hold values from -0.1875 to 0.1875
Outputs:
- attention_out: bfloat16 [4, 24576, 2048], P('dp', ('kv', 'tp'))
The draws below stay inside these ranges and needn't reach their ends.
Inputs may be any that keep to these rules, and one draw needn't show every extreme that they name: `block_picks`: A query block's entries name distinct blocks that all lie in earlier spans of 384 positions, or are -1; the largest such block is named in every draw. For one span and one group, the entries of all its query blocks together name blocks of any one other span at most 2 times; this is reached in every draw.
All inputs are finite; a program needn't handle non-finite values. No bound on the sum of `seq_lengths` on one device may be relied on, other than what follows from the above.
Results may differ from the reference program's by a relative error of at most 0.01.
The reference program's roundings to bfloat16 on the way count: a program that leaves them out, or rounds other values in their place, can miss the bound.
Values may be sent and summed in bfloat16 or wider, within the bound.
A program may use at most 64 MiB of HBM per device.

```python
import math
import jax
import jax.numpy as jnp
import numpy as np
from jax import lax

D = 2048
HEADS = 16
GROUPS = 4
HEAD = 64
BLK = 64
PICKS = 16
CAP = 2
TOK_DEV = 384
SEQS = 4
SEQ_LEN = 24576
HEAD_SETS = 2


def draw_tokens(key, part):
    grid_shape = (SEQS, SEQ_LEN, D)
    return jnp.clip(jax.random.normal(jax.random.fold_in(key, 20), grid_shape, jnp.float32), -6.0, 6.0).astype(jnp.bfloat16)


def draw_block_picks(key, part):
    span_count = SEQ_LEN // TOK_DEV
    per_span = TOK_DEV // BLK
    slot_total = per_span * PICKS
    grid_shape = (SEQS, span_count, GROUPS, span_count)
    random_order = jax.random.randint(jax.random.fold_in(key, 11), grid_shape, 0, 1 << 20)
    shifts = jax.random.randint(jax.random.fold_in(key, 12), grid_shape, 0, per_span)
    current = jnp.arange(span_count, dtype=jnp.int32)[None, :, None, None]
    candidate = jnp.arange(span_count, dtype=jnp.int32)[None, None, None, :]
    at_end = (current == span_count - 1) & (candidate == span_count - 2)
    shifts = jnp.where(at_end, per_span - 1, shifts)
    ranking = random_order * span_count + candidate
    ranking = jnp.where(candidate == 0, -3, ranking)
    ranking = jnp.where(candidate == current - 1, -4, ranking)
    ranking = jnp.where(candidate == current - span_count // 2, -1, ranking)
    ranking = jnp.where(candidate >= current, (1 << 20) * span_count + candidate, ranking)
    ordered = jnp.argsort(ranking, axis=-1).astype(jnp.int32)
    slots = jnp.arange(slot_total, dtype=jnp.int32)
    places = jnp.minimum(slots // CAP, span_count - 1)
    owners = jnp.take(ordered, places, axis=-1)
    offsets = jnp.take_along_axis(shifts, owners, axis=-1)
    inside = (offsets + slots % CAP) % per_span
    blocks = owners * per_span + inside
    is_valid = (slots // CAP)[None, None, None, :] < current
    picked = jnp.where(is_valid, blocks, -1)
    picked = picked.reshape(SEQS, span_count, GROUPS, per_span, PICKS).transpose(0, 1, 3, 2, 4)
    return picked.reshape(SEQS, span_count * per_span, GROUPS, PICKS).astype(jnp.int32)


def block_levels(own_key, shape, cuts, smallest, largest):
    gain = 1.0
    for dim, blocks in cuts:
        heights = jax.random.uniform(jax.random.fold_in(jax.random.fold_in(own_key, 6), dim), (blocks,), jnp.float32, smallest / len(cuts), largest / len(cuts))
        gain = gain * jnp.repeat(jnp.exp(heights), shape[dim] // blocks).reshape((-1,) + (1,) * (len(shape) - 1 - dim))
    return gain


def profile(number_of, total, limit, lean):
    portions = [(1 << 20) // math.isqrt(rank ** lean) + 1 for rank in range(2, number_of + 1)]
    rest, given = total - limit - (number_of - 1), [1] * (number_of - 1)
    while rest > 0:
        free = [i for i in range(number_of - 1) if given[i] < limit]
        whole, remaining = sum([portions[i] for i in free]), rest
        for i in free:
            extra = min(limit - given[i], max(1, remaining * portions[i] // whole), rest)
            given[i] = given[i] + extra
            rest = rest - extra
    return np.array([limit] + given)


def ragged(key, amount, total, reach, skew):
    if amount == 2:
        one = jax.random.randint(key, (), max(1, total - reach), min(reach, total - 1) + 1)
        return jnp.stack([one, total - one])
    tallies = jnp.asarray(profile(amount, total, reach, skew), jnp.int32)
    pairs = (amount - 1) // 2
    giver, receiver = tallies[1:1 + 2 * pairs:2], tallies[2:2 + 2 * pairs:2]
    room = jnp.minimum(giver - 1, reach - receiver)
    shifted = jax.random.randint(jax.random.fold_in(key, 1), (pairs,), 0, 1 << 20) % (room + 1)
    tallies = tallies.at[1:1 + 2 * pairs:2].set(giver - shifted).at[2:2 + 2 * pairs:2].set(receiver + shifted)
    return tallies[jax.random.permutation(jax.random.fold_in(key, 2), amount)]


def normal_values(stream_key, dims, scale, most, shards=(), held_as=jnp.bfloat16):
    drawn = scale * jax.random.normal(stream_key, dims, jnp.float32)
    if shards:
        drawn = drawn * block_levels(stream_key, dims, shards, -0.22, 0.18)
    return jnp.clip(drawn, -most, most).astype(held_as)


def setup_inputs(seed: int = 0) -> dict:
    key_of = jax.random.split(jax.random.key(seed), 11)
    tokens = draw_tokens(jax.random.fold_in(key_of[10], 71), 0)
    seq_lengths = ragged(key_of[1], SEQS, 3 * SEQS * SEQ_LEN // 8, SEQ_LEN, 2).astype(jnp.int32)
    block_picks = draw_block_picks(jax.random.fold_in(key_of[10], 71), 0)
    w_query = normal_values(key_of[3], (D, HEADS * HEAD), D ** -0.5, 0.125, ((0, 64), (1, 2)))
    w_key = normal_values(key_of[4], (D, GROUPS * HEAD), D ** -0.5, 0.125, ((0, 64), (1, 2)))
    w_value = normal_values(key_of[5], (D, GROUPS * HEAD), D ** -0.5, 0.125, ((0, 64), (1, 2)))
    w_gate = normal_values(key_of[6], (D, 2 * HEADS), D ** -0.5, 0.125)
    w_ckey = normal_values(key_of[7], (BLK * HEAD, HEAD), (BLK * HEAD) ** -0.5, 0.09375)
    w_cvalue = normal_values(key_of[8], (BLK * HEAD, HEAD), (BLK * HEAD) ** -0.5, 0.09375)
    w_out = normal_values(key_of[9], (HEADS * HEAD, D), (HEADS * HEAD) ** -0.5, 0.1875, ((0, 2), (1, 64)))
    return dict(tokens=tokens, seq_lengths=seq_lengths, block_picks=block_picks, w_query=w_query, w_key=w_key, w_value=w_value, w_gate=w_gate, w_ckey=w_ckey, w_cvalue=w_cvalue, w_out=w_out)


masked_low = -1e30


def reference(tokens, seq_lengths, block_picks, w_query, w_key, w_value, w_gate, w_ckey, w_cvalue, w_out):
    per_group = HEADS // GROUPS
    block_total = SEQ_LEN // BLK
    inv_scale = HEAD ** -0.5
    set_width = HEADS * HEAD // HEAD_SETS
    causal = jnp.arange(BLK)[None, :] <= jnp.arange(BLK)[:, None]
    block_ends = jnp.arange(block_total, dtype=jnp.int32) * BLK + (BLK - 1)
    group_ids = jnp.arange(GROUPS, dtype=jnp.int32)

    def sequence(inputs):
        token_rows, length, picked = inputs
        queries = jnp.dot(token_rows, w_query, preferred_element_type=jnp.float32).astype(jnp.bfloat16)
        queries = lax.optimization_barrier(queries).reshape(block_total, BLK, GROUPS, per_group, HEAD)
        keys_all = jnp.dot(token_rows, w_key, preferred_element_type=jnp.float32).astype(jnp.bfloat16)
        keys_all = keys_all.reshape(block_total, BLK, GROUPS, HEAD).transpose(0, 2, 1, 3)
        values_all = jnp.dot(token_rows, w_value, preferred_element_type=jnp.float32).astype(jnp.bfloat16)
        values_all = values_all.reshape(block_total, BLK, GROUPS, HEAD).transpose(0, 2, 1, 3)
        keys_all = lax.optimization_barrier(keys_all)
        values_all = lax.optimization_barrier(values_all)
        gate_all = jax.nn.sigmoid(jnp.dot(token_rows, w_gate, preferred_element_type=jnp.float32))
        gate_all = gate_all.reshape(block_total, BLK, 2, GROUPS, per_group)
        ckeys = jnp.dot(keys_all.reshape(block_total * GROUPS, BLK * HEAD), w_ckey,
                        preferred_element_type=jnp.float32).astype(jnp.bfloat16)
        cvalues = jnp.dot(values_all.reshape(block_total * GROUPS, BLK * HEAD), w_cvalue,
                          preferred_element_type=jnp.float32).astype(jnp.bfloat16)
        ckeys = lax.optimization_barrier(ckeys).reshape(block_total, GROUPS, HEAD).astype(jnp.float32)
        cvalues = lax.optimization_barrier(cvalues).reshape(block_total, GROUPS, HEAD).astype(jnp.float32)

        def attend(block_inputs):
            qblock, gblock, picked_row, block_index = block_inputs
            qfloat = qblock.astype(jnp.float32)
            query_spots = block_index * BLK + jnp.arange(BLK, dtype=jnp.int32)
            comp_score = jnp.einsum('tgpd,cgd->gtpc', qfloat, ckeys) * inv_scale
            visible = (block_ends[None, :] <= query_spots[:, None])[None, :, None, :]
            comp_score = jnp.where(visible, comp_score, masked_low)
            comp_top = jnp.max(comp_score, axis=-1, keepdims=True)
            comp_weight = jnp.where(visible, jnp.exp(comp_score - comp_top), 0.0)
            comp_sum = jnp.maximum(jnp.sum(comp_weight, axis=-1, keepdims=True), 1.0)
            comp_prob = lax.optimization_barrier((comp_weight / comp_sum).astype(jnp.bfloat16))
            comp_out = jnp.einsum('gtpc,cgd->tgpd', comp_prob.astype(jnp.float32), cvalues)
            own_keys = keys_all[block_index].astype(jnp.float32)
            own_values = values_all[block_index].astype(jnp.float32)
            usable = picked_row >= 0
            safe_picks = jnp.where(usable, picked_row, 0)
            far_keys = keys_all[safe_picks, group_ids[:, None]].reshape(GROUPS, PICKS * BLK, HEAD).astype(jnp.float32)
            far_values = values_all[safe_picks, group_ids[:, None]].reshape(GROUPS, PICKS * BLK, HEAD).astype(jnp.float32)
            own_score = jnp.einsum('tgpd,gsd->gtps', qfloat, own_keys) * inv_scale
            own_mask = causal[None, :, None, :]
            own_score = jnp.where(own_mask, own_score, masked_low)
            far_score = jnp.einsum('tgpd,gkd->gtpk', qfloat, far_keys) * inv_scale
            far_mask = jnp.repeat(usable, BLK, axis=-1)[:, None, None, :]
            far_score = jnp.where(far_mask, far_score, masked_low)
            score_top = jnp.maximum(jnp.max(own_score, axis=-1, keepdims=True),
                                    jnp.max(far_score, axis=-1, keepdims=True))
            own_weight = jnp.where(own_mask, jnp.exp(own_score - score_top), 0.0)
            far_weight = jnp.where(far_mask, jnp.exp(far_score - score_top), 0.0)
            normalizer = jnp.sum(own_weight, axis=-1, keepdims=True) + jnp.sum(far_weight, axis=-1, keepdims=True)
            own_prob = lax.optimization_barrier((own_weight / normalizer).astype(jnp.bfloat16))
            far_prob = lax.optimization_barrier((far_weight / normalizer).astype(jnp.bfloat16))
            chosen_out = (jnp.einsum('gtps,gsd->tgpd', own_prob.astype(jnp.float32), own_values)
                          + jnp.einsum('gtpk,gkd->tgpd', far_prob.astype(jnp.float32), far_values))
            mixed_out = gblock[:, 0, :, :, None] * comp_out + gblock[:, 1, :, :, None] * chosen_out
            return mixed_out.astype(jnp.bfloat16)

        attended = lax.map(attend, (queries, gate_all, picked, jnp.arange(block_total, dtype=jnp.int32)))
        attended = attended.reshape(SEQ_LEN, HEAD_SETS, set_width)
        weight_sets = w_out.reshape(HEAD_SETS, set_width, D)
        summed = jnp.zeros((SEQ_LEN, D), jnp.float32)
        for set_index in range(HEAD_SETS):
            partial_out = jnp.dot(attended[:, set_index], weight_sets[set_index],
                                  preferred_element_type=jnp.float32).astype(jnp.bfloat16)
            summed = summed + lax.optimization_barrier(partial_out).astype(jnp.float32)
        live_rows = jnp.arange(SEQ_LEN, dtype=jnp.int32) < length
        return jnp.where(live_rows[:, None], summed, 0.0).astype(jnp.bfloat16)

    return lax.map(sequence, (tokens, seq_lengths, block_picks))
```

```python
import functools

import jax
import jax.numpy as jnp
from jax import lax
from jax.experimental import pallas as pl
from jax.experimental.pallas import tpu as pltpu
from jax.sharding import PartitionSpec as P

MESH = pl.DeviceIdType.MESH

HEADS = 16
GROUPS = 4
PER = 4
HEAD = 64
BLK = 64
PICKS = 16
N = 8
ROWS = 208
HALF = 192
SPLIT = 112
MASKED = -1e30
VMEM = pltpu.MemorySpace.VMEM
SMEM = pltpu.MemorySpace.SMEM
HBM = pltpu.MemorySpace.HBM


def place():
    kv = lax.axis_index("kv")
    return kv // N, lax.rem(kv, N)


class Copies:
    def __init__(self, send_sems, recv_sems):
        self.send_sems, self.recv_sems, self.used, self.sent = send_sems, recv_sems, 0, []

    def slot(self):
        self.used += 1
        return self.used - 1

    def send(self, i, src, dst, device):
        copy = pltpu.make_async_remote_copy(
            src_ref=src,
            dst_ref=dst,
            send_sem=self.send_sems.at[i],
            recv_sem=self.recv_sems.at[i],
            device_id=device,
            device_id_type=MESH,
        )
        copy.start()

    def arrived(self, i, ref, device):
        pltpu.make_async_remote_copy(
            src_ref=ref,
            dst_ref=ref,
            send_sem=self.send_sems.at[i],
            recv_sem=self.recv_sems.at[i],
            device_id=device,
            device_id_type=MESH,
        ).wait_recv()

    def left(self, i, ref, device):
        pltpu.make_async_remote_copy(
            src_ref=ref,
            dst_ref=ref,
            send_sem=self.send_sems.at[i],
            recv_sem=self.recv_sems.at[i],
            device_id=device,
            device_id_type=MESH,
        ).wait_send()


def when(cond, fn):
    if cond is True:
        fn()
    elif cond is not False:
        pl.when(cond)(fn)


def both(a, b):
    if a is True:
        return b
    if b is True:
        return a
    if a is False or b is False:
        return False
    return jnp.logical_and(a, b)


def wrap(i):
    return lax.rem(i + N, N)


def barrier(kinds):
    sem = pltpu.get_barrier_semaphore()
    for device in kinds:
        pl.semaphore_signal(sem, inc=1, device_id=device, device_id_type=MESH)
    pl.semaphore_wait(sem, len(kinds))


def plane_partners(z, y):
    return [{"kv": z * N + wrap(y + d)} for d in range(1, N)] + [
        {"kv": wrap(z + d) * N + y} for d in range(1, N)
    ]


class Gather:
    def __init__(self, copies, src, view, rows, causal, pair):
        self.c, self.src, self.view, self.rows, self.causal, self.pair = (
            copies,
            src,
            view,
            rows,
            causal,
            pair,
        )
        self.z, self.y = place()
        self.live = True if rows == N else self.z < rows
        self.waits = []
        self.pair_waits = []
        self.pending = []

    def dev(self, z, y):
        return {"kv": z * N + y}

    def transfer(self, cond_send, src, dst, device, cond_recv, got):
        i = self.c.slot()
        when(cond_send, lambda: self.c.send(i, src, dst, device))
        self.waits.append((i, cond_send, src, device))
        return (i, cond_recv, got, device)

    def take(self, t):
        i, cond, ref, device = t
        when(cond, lambda: self.c.arrived(i, ref, device))

    def mirror(self, cond, ref):
        if self.pair is None:
            return
        i = self.c.slot()
        when(cond, lambda: self.c.send(i, ref, ref, self.pair))
        self.pair_waits.append((i, cond, ref))

    def first(self):
        z, y = self.z, self.y
        self.a1, self.b1 = [], []
        for d in range(1, N):
            self.a1.append(
                self.transfer(
                    self.live,
                    self.src(0),
                    self.view(z, 1, y, 1, 0),
                    self.dev(z, wrap(y + d)),
                    self.live,
                    self.view(z, 1, wrap(y - d), 1, 0),
                )
            )
        for d in range(1, N) if not self.causal else range(1, self.rows):
            cs = True if not self.causal else z + d < self.rows
            cr = True if not self.causal else both(self.live, z - d >= 0)
            self.b1.append(
                self.transfer(
                    cs,
                    self.src(1),
                    self.view(z, 1, y, 1, 1),
                    self.dev(wrap(z + d), y),
                    cr,
                    self.view(wrap(z - d), 1, y, 1, 1),
                )
            )

    def hop_a(self, right, sub, k, depth):
        z, y = self.z, self.y
        y0, ny = (sub * 4, 4)
        if right:
            o, got, to = wrap(z - (k - 1)), wrap(z - k), wrap(z + 1)
            cs = both(z - (k - 1) >= 0, z + 1 < self.rows) if self.causal else True
            cr = both(self.live, z - k >= 0) if self.causal else True
        else:
            o, got, to = wrap(z + k - 1), lax.rem(z + k, N), wrap(z - 1)
            cs = o < depth if self.causal else True
            cr = got < depth if self.causal else True
        return self.transfer(
            cs,
            self.view(o, 1, y0, ny, 0),
            self.view(o, 1, y0, ny, 0),
            self.dev(to, y),
            cr,
            self.view(got, 1, y0, ny, 0),
        )

    def hop_b(self, right, sub, k):
        z, y = self.z, self.y
        if self.rows == N:
            z0, nz = sub * 4, 4
            cond = True if (sub == 0 or not self.causal) else z >= 4
        else:
            z0, nz = 0, self.rows
            cond = self.live
        if right:
            o, got, to = wrap(y - (k - 1)), wrap(y - k), wrap(y + 1)
        else:
            o, got, to = lax.rem(y + k - 1, N), lax.rem(y + k, N), wrap(y - 1)
        return self.transfer(
            cond,
            self.view(z0, nz, o, 1, 1),
            self.view(z0, nz, o, 1, 1),
            self.dev(z, to),
            cond,
            self.view(z0, nz, got, 1, 1),
        )

    def depth_a(self, right, sub):
        if self.rows < N:
            return self.rows - 1 if right else 0
        return 4 if right == (sub == 0) else 3

    def depth_b(self, right, sub):
        if self.rows < N and sub == 1:
            return 0
        return 4 if right == (sub == 0) else 3

    def lanes(self):
        return [(r, s) for s in (0, 1) for r in (True, False)]

    def hop(self, k):
        if k == 1:
            self.flight = {}
        for ring in ("a", "b"):
            if k == 1:
                for t in self.a1 if ring == "a" else self.b1:
                    self.take(t)
            for r, s in self.lanes():
                depth = self.depth_a(r, s) if ring == "a" else self.depth_b(r, s)
                if k > 1 and k - 1 <= depth:
                    t = self.flight[ring, r, s]
                    self.take(t)
                    self.pending.append((t[1], t[2]))
                if k <= depth:
                    self.flight[ring, r, s] = (
                        self.hop_a(r, s, k, depth) if ring == "a" else self.hop_b(r, s, k)
                    )
            if k == 1:
                if ring == "a":
                    self.pending.append((self.live, self.view(self.z, 1, 0, N, 0)))
                else:
                    self.pending.append(
                        (self.live, self.view(0, N if self.rows == N else self.rows, self.y, 1, 1))
                    )
        for cond, ref in self.pending:
            self.mirror(cond, ref)
        self.pending = []

    def last(self):
        for i, cond, ref in self.pair_waits:
            when(cond, lambda: self.c.arrived(i, ref, self.pair))
            when(cond, lambda: self.c.left(i, ref, self.pair))
        for i, cond, ref, device in self.waits:
            when(cond, lambda: self.c.left(i, ref, device))


def weights_kernel(src_ref, out_ref, send_sems, recv_sems):
    z, y = place()
    rows, cols = src_ref.shape
    half = cols // 2
    barrier(plane_partners(z, y))
    out_ref[z, y] = src_ref[...]
    c = Copies(send_sems, recv_sems)

    def src(part):
        return src_ref.at[:, pl.ds(part * half, half)]

    def view(z0, nz, y0, ny, part):
        zi = z0 if nz == 1 else pl.ds(z0, nz)
        yi = y0 if ny == 1 else pl.ds(y0, ny)
        return out_ref.at[zi, yi, :, pl.ds(part * half, half)]

    g = Gather(c, src, view, N, False, None)
    g.first()
    for k in range(1, 6):
        g.hop(k)
    g.last()


def gather_weights(piece):
    rows, cols = piece.shape
    return pl.pallas_call(
        weights_kernel,
        out_shape=jax.ShapeDtypeStruct((N, N, rows, cols), piece.dtype),
        in_specs=[pl.BlockSpec(memory_space=VMEM)],
        out_specs=pl.BlockSpec(memory_space=VMEM),
        scratch_shapes=[pltpu.SemaphoreType.DMA((64,)), pltpu.SemaphoreType.DMA((64,))],
        compiler_params=pltpu.CompilerParams(
            collective_id=0, has_side_effects=True, vmem_limit_bytes=24 << 20
        ),
        name="gather_weights",
    )(piece)


def spread_kernel(main_ref, ints_ref, got_ref, gint_ref, send_sems, recv_sems):
    dp, tp = lax.axis_index("dp"), lax.axis_index("tp")
    others = []
    for e in range(1, 8):
        d, t = e // 2, e % 2
        others.append({"dp": lax.rem(dp + d, 4), "tp": lax.rem(tp + t, 2)})
    barrier(others)
    c = Copies(send_sems, recv_sems)
    mine = dp // 2 == tp
    for gl in range(2):
        for h in range(2):
            g = 2 * tp + gl
            own = jnp.logical_and(g == dp, tp == h)
            device = {"dp": g, "tp": jnp.int32(h)}
            i = (gl * 2 + h) * 2

            def go(gl=gl, h=h, device=device):
                for k, (s, d) in enumerate(((main_ref, got_ref), (ints_ref, gint_ref))):
                    pltpu.make_async_remote_copy(
                        src_ref=s.at[gl, h],
                        dst_ref=d.at[dp],
                        send_sem=send_sems.at[(gl * 2 + h) * 2 + k],
                        recv_sem=recv_sems.at[dp, k],
                        device_id=device,
                        device_id_type=MESH,
                    ).start()

            def keep(gl=gl, h=h):
                got_ref[dp] = main_ref[gl, h]
                gint_ref[dp] = ints_ref[gl, h]

            pl.when(jnp.logical_not(own))(go)
            pl.when(own)(keep)
    for q in range(4):
        theirs = jnp.logical_not(jnp.logical_and(q == dp, mine))

        def take(q=q):
            for k, d in enumerate((got_ref, gint_ref)):
                pltpu.make_async_remote_copy(
                    src_ref=d.at[q],
                    dst_ref=d.at[q],
                    send_sem=send_sems.at[k],
                    recv_sem=recv_sems.at[q, k],
                    device_id={"dp": jnp.int32(q), "tp": tp},
                    device_id_type=MESH,
                ).wait_recv()

        pl.when(theirs)(take)
    for gl in range(2):
        for h in range(2):
            g = 2 * tp + gl
            own = jnp.logical_and(g == dp, tp == h)

            def done(gl=gl, h=h, g=g):
                for k, s in enumerate((main_ref, ints_ref)):
                    pltpu.make_async_remote_copy(
                        src_ref=s.at[gl, h],
                        dst_ref=s.at[gl, h],
                        send_sem=send_sems.at[(gl * 2 + h) * 2 + k],
                        recv_sem=recv_sems.at[0, k],
                        device_id={"dp": g, "tp": jnp.int32(h)},
                        device_id_type=MESH,
                    ).wait_send()

            pl.when(jnp.logical_not(own))(done)


def spread(main, ints):
    return pl.pallas_call(
        spread_kernel,
        out_shape=[
            jax.ShapeDtypeStruct((4,) + main.shape[2:], main.dtype),
            jax.ShapeDtypeStruct((4,) + ints.shape[2:], ints.dtype),
        ],
        in_specs=[pl.BlockSpec(memory_space=VMEM)] * 2,
        out_specs=[pl.BlockSpec(memory_space=VMEM)] * 2,
        scratch_shapes=[pltpu.SemaphoreType.DMA((8,)), pltpu.SemaphoreType.DMA((4, 2))],
        compiler_params=pltpu.CompilerParams(
            collective_id=1, has_side_effects=True, vmem_limit_bytes=16 << 20
        ),
        name="spread",
    )(main, ints)


def kv_kernel(spans, src_ref, *refs):
    outs, (send_sems, recv_sems) = refs[: len(spans)], refs[len(spans) :]
    z, y = place()
    tp = lax.axis_index("tp")
    pair = {"tp": 1 - tp}
    barrier(plane_partners(z, y) + [pair])
    c = Copies(send_sems, recv_sems)
    jobs = []
    for r, rows in enumerate(spans):
        out_ref = outs[r]

        def own(out_ref=out_ref, r=r):
            out_ref[tp, z, y] = src_ref[r]

        when(True if rows == N else z < rows, own)

        def src(part, r=r):
            return src_ref.at[r, pl.ds(0, SPLIT) if part == 0 else pl.ds(SPLIT, ROWS - SPLIT)]

        def view(z0, nz, y0, ny, part, out_ref=out_ref):
            zi = z0 if nz == 1 else pl.ds(z0, nz)
            yi = y0 if ny == 1 else pl.ds(y0, ny)
            rows_of = pl.ds(0, SPLIT) if part == 0 else pl.ds(SPLIT, ROWS - SPLIT)
            return out_ref.at[tp, zi, yi, rows_of]

        jobs.append(Gather(c, src, view, rows, True, pair))
    for g in jobs:
        g.first()
    for k in range(1, 6):
        for g in jobs:
            g.hop(k)
    for g in jobs:
        g.last()


def gather_kv(src, spans, number):
    return pl.pallas_call(
        functools.partial(kv_kernel, spans),
        out_shape=[jax.ShapeDtypeStruct((2, rows, N, ROWS, 2 * HEAD), src.dtype) for rows in spans],
        in_specs=[pl.BlockSpec(memory_space=VMEM)],
        out_specs=[pl.BlockSpec(memory_space=VMEM)] * len(spans),
        scratch_shapes=[pltpu.SemaphoreType.DMA((320,)), pltpu.SemaphoreType.DMA((320,))],
        compiler_params=pltpu.CompilerParams(
            collective_id=number, has_side_effects=True, vmem_limit_bytes=40 << 20
        ),
        name="gather_kv",
    )(src)


def attend_kernel(spans, order_ref, lens_ref, picks_ref, main_ref, gate_ref, bias_ref, comp_ref, *refs):
    kv_refs, (out_ref, buf, sems) = refs[: len(spans)], refs[len(spans) :]
    kv, tp = lax.axis_index("kv"), lax.axis_index("tp")
    start = kv * (2 * HALF) + tp * HALF
    for r, rows in enumerate(spans):
        seq = order_ref[r]

        @pl.when(jnp.logical_and(start < lens_ref[seq], kv < rows * N))
        def _(r=r, seq=seq):
            def fetch(n, carry):
                j = n // PICKS
                p = lax.rem(n, PICKS)
                b = jnp.maximum(picks_ref[seq, j, p], 0)
                span = b // 6
                at = b - span * 6
                t = at // 3
                row = (at - t * 3) * BLK
                pltpu.make_async_copy(
                    kv_refs[r].at[t, span // N, lax.rem(span, N), pl.ds(pl.multiple_of(row, BLK), BLK)],
                    buf.at[r * 3 + j, pl.ds(pl.multiple_of(p * BLK, BLK), BLK)],
                    sems.at[r * 3 + j],
                ).start()
                return carry

            lax.fori_loop(0, 3 * PICKS, fetch, 0)

    lane = lax.broadcasted_iota(jnp.int32, (BLK, 128), 1)
    row_in = lax.rem(lax.broadcasted_iota(jnp.int32, (PER * BLK, 1), 0), BLK)

    def step(n, carry):
        r = n // 3
        j = n - r * 3
        seq = order_ref[r]
        rows = pl.ds(pl.multiple_of(j * BLK, BLK), BLK)
        live = start < lens_ref[seq]

        @pl.when(jnp.logical_not(live))
        def _():
            out_ref[seq, rows] = jnp.zeros((BLK, PER * HEAD), jnp.bfloat16)

        @pl.when(live)
        def _():
            pltpu.make_async_copy(buf.at[n], buf.at[n], sems.at[n]).wait()
            parts = []
            for h in range(PER):
                two = main_ref[seq, rows, pl.ds((h // 2) * 128, 128)].astype(jnp.float32) * 0.125
                if h % 2:
                    two = pltpu.roll(two, 64, 1)
                parts.append(jnp.where(lane < HEAD, two, 0.0).astype(jnp.bfloat16))
            q = jnp.concatenate(parts, axis=0)

            def score(keys):
                return lax.dot_general(
                    q, keys, (((1,), (1,)), ((), ())), preferred_element_type=jnp.float32
                )

            spot = start + j * BLK + row_in
            comp = comp_ref[r]
            ends = lax.broadcasted_iota(jnp.int32, (1, comp.shape[0]), 1) * BLK + (BLK - 1)
            seen = ends <= spot
            cs = jnp.where(seen, score(comp), MASKED)
            ctop = jnp.max(cs, axis=-1, keepdims=True)
            cw = jnp.where(seen, jnp.exp(cs - ctop), 0.0)
            cn = jnp.maximum(jnp.sum(cw, axis=-1, keepdims=True), 1.0)
            cp = (cw * (1.0 / cn)).astype(jnp.bfloat16)
            co = jnp.dot(cp, comp, preferred_element_type=jnp.float32)

            own = main_ref[seq, rows, pl.ds(PER * HEAD, 128)]
            far = buf[n]
            ks = lax.broadcasted_iota(jnp.int32, (1, BLK), 1)
            os = jnp.where(ks <= row_in, score(own), MASKED)
            fs = jnp.where(bias_ref[seq, j] > 0.5, score(far), MASKED)
            top = jnp.maximum(
                jnp.max(os, axis=-1, keepdims=True), jnp.max(fs, axis=-1, keepdims=True)
            )
            ow, fw = jnp.exp(os - top), jnp.exp(fs - top)
            inv = 1.0 / (jnp.sum(ow, axis=-1, keepdims=True) + jnp.sum(fw, axis=-1, keepdims=True))
            so = jnp.dot(
                (ow * inv).astype(jnp.bfloat16), own, preferred_element_type=jnp.float32
            ) + jnp.dot((fw * inv).astype(jnp.bfloat16), far, preferred_element_type=jnp.float32)
            mixed = []
            gates = gate_ref[seq, rows]
            for h in range(PER):
                at = slice(h * BLK, (h + 1) * BLK)
                mixed.append(gates[:, h : h + 1] * co[at] + gates[:, 4 + h : 5 + h] * so[at])
            for h in range(2):
                pair = jnp.where(lane < HEAD, pltpu.roll(mixed[2 * h], 64, 1), mixed[2 * h + 1])
                out_ref[seq, rows, pl.ds(h * 128, 128)] = pair.astype(jnp.bfloat16)

        return carry

    lax.fori_loop(0, 12, step, 0)


def attend(spans, order, lens, picks, main, gates, bias, comp, gathered):
    vm = pl.BlockSpec(memory_space=VMEM)
    sm = pl.BlockSpec(memory_space=SMEM)
    return pl.pallas_call(
        functools.partial(attend_kernel, spans),
        out_shape=jax.ShapeDtypeStruct((4, HALF, PER * HEAD), jnp.bfloat16),
        in_specs=[sm, sm, sm, vm, vm, vm, vm] + [pl.BlockSpec(memory_space=HBM)] * len(spans),
        out_specs=vm,
        scratch_shapes=[
            pltpu.VMEM((12, PICKS * BLK, 2 * HEAD), jnp.bfloat16),
            pltpu.SemaphoreType.DMA((12,)),
        ],
        compiler_params=pltpu.CompilerParams(vmem_limit_bytes=32 << 20),
        name="attend",
    )(order, lens, picks, main, gates, bias, comp, *gathered)


def by_halves(a):
    return a.reshape(2, HALF, *a.shape[1:])


def body(
    tokens, seq_lengths, block_picks, w_query, w_key, w_value, w_gate, w_ckey, w_cvalue, w_out
):
    x = tokens[0]
    kv, tp, dp = lax.axis_index("kv"), lax.axis_index("tp"), lax.axis_index("dp")
    piece = jnp.concatenate(
        [
            w_query[:, :256],
            w_key[:, :64],
            w_value[:, :64],
            w_query[:, 256:],
            w_key[:, 64:],
            w_value[:, 64:],
        ],
        axis=1,
    )
    w_all = gather_weights(piece).reshape(2048, 768)
    out_w = lax.all_gather(w_out, "kv", axis=1, tiled=True)
    out_w = lax.all_gather(out_w, "tp", axis=0, tiled=True)

    gate_all = jax.nn.sigmoid(jnp.dot(x, w_gate, preferred_element_type=jnp.float32))
    gate_all = gate_all.reshape(384, 2, 2, 2, PER)
    gate_own = lax.dynamic_index_in_dim(gate_all, tp, 2, keepdims=False)
    gate_own = gate_own.transpose(2, 1, 3, 0).reshape(2, 8, 2, HALF).transpose(0, 2, 1, 3)
    hi = gate_own.astype(jnp.bfloat16)
    lo = (gate_own - hi.astype(jnp.float32)).astype(jnp.bfloat16)
    gate_rows = jnp.concatenate([hi, lo], axis=2)
    gate_rows = jnp.pad(gate_rows, ((0, 0), (0, 0), (0, 0), (0, 64)))

    qkv = jnp.dot(x, w_all, preferred_element_type=jnp.float32).astype(jnp.bfloat16)
    mains = []
    for gl in range(2):
        one = qkv[:, gl * 384 : (gl + 1) * 384]
        ck = jnp.dot(
            one[:, 256:320].reshape(6, BLK * HEAD), w_ckey, preferred_element_type=jnp.float32
        )
        cv = jnp.dot(
            one[:, 320:384].reshape(6, BLK * HEAD), w_cvalue, preferred_element_type=jnp.float32
        )
        pairs = jnp.concatenate([ck, cv], axis=1).astype(jnp.bfloat16).reshape(2, 3, 128)
        pairs = jnp.pad(pairs, ((0, 0), (0, 13), (0, 0)))
        extra = jnp.concatenate([gate_rows[gl], pairs], axis=2)
        mains.append(jnp.concatenate([by_halves(one), extra], axis=1))
    main = jnp.stack(mains)

    picks = block_picks[0].transpose(1, 0, 2).reshape(2, 2, 3, PICKS)
    ints = jnp.pad(picks, ((0, 0), (0, 0), (0, 5), (0, 112)))
    row = lax.broadcasted_iota(jnp.int32, ints.shape, 2)
    ints = jnp.where(row == 7, seq_lengths[0], ints)

    got, gint = spread(main, ints)
    lens = gint[:, 7, 0]
    ids = jnp.arange(4, dtype=jnp.int32)
    ahead = (lens[None, :] > lens[:, None]) | (
        (lens[None, :] == lens[:, None]) & (ids[None, :] < ids[:, None])
    )
    rank = jnp.sum(ahead.astype(jnp.int32), axis=1)
    order = jnp.sum(jnp.where(rank[None, :] == ids[:, None], ids[None, :], 0), axis=1)
    ranked = jnp.sum(
        jnp.where(rank[None, :] == ids[:, None], lens[None, :], 0), axis=1
    )
    pieces = got[:, :, 256:384]
    src = jnp.stack([lax.dynamic_index_in_dim(pieces, order[r], 0, keepdims=False) for r in range(4)])
    sel = gint[:, :3, :PICKS]
    bias = jnp.repeat((sel >= 0).astype(jnp.float32), BLK, axis=2).reshape(4, 3, 1, PICKS * BLK)
    both_parts = got[:, HALF:ROWS, :HALF].astype(jnp.float32)
    gates = (both_parts[:, :8] + both_parts[:, 8:]).transpose(0, 2, 1)

    def run(spans, number):
        gathered = gather_kv(src, spans, number)
        comp = []
        for rows, g in zip(spans, gathered):
            c = g[:, :, :, HALF : HALF + 3].reshape(2, rows * N, 3, 128)
            c = c.transpose(1, 0, 2, 3).reshape(rows * N * 6, 128)
            at = jnp.arange(rows * N * 6, dtype=jnp.int32)[:, None] // 6
            c = jnp.where(at <= kv, c, jnp.zeros_like(c))
            comp.append(jnp.pad(c, ((0, 384 - rows * N * 6), (0, 0))))
        return attend(spans, order, lens, sel, got, gates, bias, jnp.stack(comp), gathered)

    span = N * 384
    small = (ranked[1] <= 3 * span) & (ranked[2] <= 2 * span)
    att = lax.cond(small, lambda: run((8, 3, 2, 2), 2), lambda: run((8, 8, 8, 8), 3))

    back = lax.all_to_all(att, "dp", split_axis=0, concat_axis=0, tiled=True)
    summed = jnp.zeros((HALF, 2048), jnp.float32)
    for s in range(2):
        cols = jnp.concatenate([back[2 * s], back[2 * s + 1]], axis=1)
        summed = summed + jnp.dot(
            cols, out_w[s * 512 : (s + 1) * 512], preferred_element_type=jnp.float32
        ).astype(jnp.bfloat16).astype(jnp.float32)
    spots = kv * 384 + tp * HALF + jnp.arange(HALF, dtype=jnp.int32)
    alive = spots < seq_lengths[0]
    return jnp.where(alive[:, None], summed, 0.0).astype(jnp.bfloat16)[None]


def solution(mesh):
    return jax.shard_map(
        body,
        mesh=mesh,
        in_specs=(
            P("dp", "kv", None),
            P("dp"),
            P("dp", "kv", "tp", None),
            P("kv", "tp"),
            P("kv", "tp"),
            P("kv", "tp"),
            P(),
            P(),
            P(),
            P("tp", "kv"),
        ),
        out_specs=P("dp", ("kv", "tp"), None),
        check_vma=False,
    )
```

```python
import functools

import jax
import jax.numpy as jnp
from jax import lax
from jax.experimental import pallas as pl
from jax.experimental.pallas import tpu as pltpu
from jax.sharding import PartitionSpec as P

MESH = pl.DeviceIdType.MESH

HEADS = 16
GROUPS = 4
PER = 4
HEAD = 64
BLK = 64
PICKS = 16
N = 8
ROWS = 208
HALF = 192
SPLIT = 112
MASKED = -1e30
VMEM = pltpu.MemorySpace.VMEM
SMEM = pltpu.MemorySpace.SMEM
HBM = pltpu.MemorySpace.HBM


def place():
    kv = lax.axis_index("kv")
    return kv // N, lax.rem(kv, N)


class Copies:
    def __init__(self, send_sems, recv_sems):
        self.send_sems, self.recv_sems, self.used, self.sent = send_sems, recv_sems, 0, []

    def slot(self):
        self.used += 1
        return self.used - 1

    def send(self, i, src, dst, device):
        copy = pltpu.make_async_remote_copy(
            src_ref=src,
            dst_ref=dst,
            send_sem=self.send_sems.at[i],
            recv_sem=self.recv_sems.at[i],
            device_id=device,
            device_id_type=MESH,
        )
        copy.start()

    def arrived(self, i, ref, device):
        pltpu.make_async_remote_copy(
            src_ref=ref,
            dst_ref=ref,
            send_sem=self.send_sems.at[i],
            recv_sem=self.recv_sems.at[i],
            device_id=device,
            device_id_type=MESH,
        ).wait_recv()

    def left(self, i, ref, device):
        pltpu.make_async_remote_copy(
            src_ref=ref,
            dst_ref=ref,
            send_sem=self.send_sems.at[i],
            recv_sem=self.recv_sems.at[i],
            device_id=device,
            device_id_type=MESH,
        ).wait_send()


def when(cond, fn):
    if cond is True:
        fn()
    elif cond is not False:
        pl.when(cond)(fn)


def both(a, b):
    if a is True:
        return b
    if b is True:
        return a
    if a is False or b is False:
        return False
    return jnp.logical_and(a, b)


def wrap(i):
    return lax.rem(i + N, N)


def barrier(kinds):
    sem = pltpu.get_barrier_semaphore()
    for device in kinds:
        pl.semaphore_signal(sem, inc=1, device_id=device, device_id_type=MESH)
    pl.semaphore_wait(sem, len(kinds))


def plane_partners(z, y):
    return [{"kv": z * N + wrap(y + d)} for d in range(1, N)] + [
        {"kv": wrap(z + d) * N + y} for d in range(1, N)
    ]


class Gather:
    def __init__(self, copies, src, view, rows, causal, pair, parts=(True, True), tie=False):
        self.c, self.src, self.view, self.rows, self.causal = copies, src, view, rows, causal
        self.pair, self.parts, self.tie = pair, parts, tie
        self.z, self.y = place()
        self.live = True if rows == N else self.z < rows
        self.waits = []
        self.pair_waits = []
        self.flight = {}
        if not causal:
            self.subs_b = [(0, 4), (4, 4)]
        elif rows == N:
            self.subs_b = [(0, 1), (1, 1), (2, 2), (4, 2), (6, 2)]
        else:
            self.subs_b = [(i, 1) for i in range(rows)]

    def dev(self, z, y):
        return {"kv": z * N + y}

    def transfer(self, cond_send, src, dst, device, cond_recv, got):
        i = self.c.slot()
        when(cond_send, lambda: self.c.send(i, src, dst, device))
        self.waits.append((i, cond_send, src, device))
        return (i, cond_recv, got, device)

    def take(self, t):
        i, cond, ref, device = t
        when(cond, lambda: self.c.arrived(i, ref, device))

    def mirror(self, cond, ref):
        if self.pair is None:
            return
        i = self.c.slot()
        when(cond, lambda: self.c.send(i, ref, ref, self.pair))
        self.pair_waits.append((i, cond, ref))

    def first(self):
        z, y = self.z, self.y
        self.a1, self.b1 = [], []
        for d in range(1, N) if self.parts[0] else ():
            self.a1.append(
                self.transfer(
                    self.live,
                    self.src(0),
                    self.view(z, 1, y, 1, 0),
                    self.dev(z, wrap(y + d)),
                    self.live,
                    self.view(z, 1, wrap(y - d), 1, 0),
                )
            )
        reach = N if not self.causal else self.rows
        for d in range(1, reach) if self.parts[1] else ():
            cs = True if not self.causal else z + d < self.rows
            cr = True if not self.causal else both(self.live, z - d >= 0)
            self.b1.append(
                self.transfer(
                    cs,
                    self.src(1),
                    self.view(z, 1, y, 1, 1),
                    self.dev(wrap(z + d), y),
                    cr,
                    self.view(wrap(z - d), 1, y, 1, 1),
                )
            )

    def ring_y(self, k, z0, nz, part, right, cond):
        z, y = self.z, self.y
        if right:
            o, got, to = wrap(y - (k - 1)), wrap(y - k), wrap(y + 1)
        else:
            o, got, to = lax.rem(y + k - 1, N), lax.rem(y + k, N), wrap(y - 1)
        return self.transfer(
            cond,
            self.view(z0, nz, o, 1, part),
            self.view(z0, nz, o, 1, part),
            self.dev(z, to),
            cond,
            self.view(z0, nz, got, 1, part),
        )

    def hop_a(self, right, sub, k, depth):
        z, y = self.z, self.y
        y0, ny = (sub * 4, 4)
        if right:
            o, got, to = wrap(z - (k - 1)), wrap(z - k), wrap(z + 1)
            cs = both(z - (k - 1) >= 0, z + 1 < self.rows) if self.causal else True
            cr = both(self.live, z - k >= 0) if self.causal else True
        else:
            o, got, to = wrap(z + k - 1), lax.rem(z + k, N), wrap(z - 1)
            cs = o < depth if self.causal else True
            cr = got < depth if self.causal else True
        return self.transfer(
            cs,
            self.view(o, 1, y0, ny, 0),
            self.view(o, 1, y0, ny, 0),
            self.dev(to, y),
            cr,
            self.view(got, 1, y0, ny, 0),
        )

    def hop_b(self, right, sub, k):
        z0, nz = self.subs_b[sub]
        cond = self.live
        if self.causal and z0 > 0:
            cond = both(cond, self.z >= z0)
        return self.ring_y(k, z0, nz, 1, right, cond)

    def depth_a(self, right, sub):
        if self.rows < N:
            return self.rows - 1 if right else 0
        return 4 if right == (sub == 0) else 3

    def depth_b(self, right, sub):
        return 4 if right == ((sub % 2 == 0) != self.tie) else 3

    def hop(self, k):
        steps = []
        order = [("a", 0), ("b", 0), ("b", 1), ("a", 1)] + [("b", i) for i in range(2, 5)]
        begun = set()
        for ring, s in order:
            if s >= (2 if ring == "a" else len(self.subs_b)) or not self.parts[ring == "b"]:
                continue
            if k == 1 and ring not in begun:
                begun.add(ring)
                steps.append(lambda ring=ring: self.begin(ring))
            for r in (True, False):
                steps.append(lambda ring=ring, s=s, r=r: self.lane(ring, s, r, k))
        return steps

    def begin(self, ring):
        for t in self.a1 if ring == "a" else self.b1:
            self.take(t)

    def lane(self, ring, s, r, k):
        depth = self.depth_a(r, s) if ring == "a" else self.depth_b(r, s)
        got = None
        if 1 < k <= depth + 1:
            got = self.flight[ring, r, s]
            self.take(got)
        if k <= depth:
            self.flight[ring, r, s] = (
                self.hop_a(r, s, k, depth) if ring == "a" else self.hop_b(r, s, k)
            )
        if got is not None:
            self.mirror(got[1], got[2])
        if k == 1 and r:
            if ring == "a":
                self.mirror(self.live, self.view(self.z, 1, s * 4, 4, 0))
            else:
                z0, nz = self.subs_b[s]
                cond = both(self.live, self.z >= z0) if z0 else self.live
                self.mirror(cond, self.view(z0, nz, self.y, 1, 1))

    def last(self):
        for i, cond, ref in self.pair_waits:
            when(cond, lambda: self.c.arrived(i, ref, self.pair))
            when(cond, lambda: self.c.left(i, ref, self.pair))
        for i, cond, ref, device in self.waits:
            when(cond, lambda: self.c.left(i, ref, device))


def weights_kernel(*refs):
    srcs, outs, (send_sems, recv_sems) = refs[:2], refs[2:4], refs[4:]
    z, y = place()
    for src_ref, out_ref in zip(srcs, outs):
        out_ref[z, y] = src_ref[...]
    barrier(plane_partners(z, y))
    c = Copies(send_sems, recv_sems)
    jobs = []
    for src_ref, out_ref in zip(srcs, outs):
        half = src_ref.shape[0] // 2

        def src(part, src_ref=src_ref, half=half):
            return src_ref.at[pl.ds(part * half, half)]

        def view(z0, nz, y0, ny, part, out_ref=out_ref, half=half):
            zi = z0 if nz == 1 else pl.ds(z0, nz)
            yi = y0 if ny == 1 else pl.ds(y0, ny)
            return out_ref.at[zi, yi, pl.ds(part * half, half)]

        jobs.append(Gather(c, src, view, N, False, None))
    for g in jobs:
        g.first()
    for k in range(1, 6):
        for g in jobs:
            for step in g.hop(k):
                step()
    for g in jobs:
        g.last()


def gather_weights(*pieces):
    vm = pl.BlockSpec(memory_space=VMEM)
    return pl.pallas_call(
        weights_kernel,
        out_shape=[jax.ShapeDtypeStruct((N, N) + p.shape, p.dtype) for p in pieces],
        in_specs=[vm, vm],
        out_specs=[vm, vm],
        scratch_shapes=[pltpu.SemaphoreType.DMA((96,)), pltpu.SemaphoreType.DMA((96,))],
        compiler_params=pltpu.CompilerParams(
            collective_id=0, has_side_effects=True, vmem_limit_bytes=24 << 20
        ),
        name="gather_weights",
    )(*pieces)


def spread_partners(dp, tp):
    return [
        {"dp": lax.rem(dp + e // 2, 4), "tp": lax.rem(tp + e % 2, 2)} for e in range(1, 8)
    ]


def spread_kernel(main_ref, ints_ref, got_ref, gint_ref, send_sems, recv_sems):
    dp, tp = lax.axis_index("dp"), lax.axis_index("tp")
    barrier(spread_partners(dp, tp))
    pairs = ((main_ref, got_ref), (ints_ref, gint_ref))

    def copy(gl, h, k):
        s, d = pairs[k]
        return pltpu.make_async_remote_copy(
            src_ref=s.at[gl, h],
            dst_ref=d.at[dp],
            send_sem=send_sems.at[(gl * 2 + h) * 2 + k],
            recv_sem=recv_sems.at[dp, k],
            device_id={"dp": 2 * tp + gl, "tp": jnp.int32(h)},
            device_id_type=MESH,
        )

    def is_own(gl, h):
        return jnp.logical_and(2 * tp + gl == dp, tp == h)

    for gl in range(2):
        for h in range(2):

            def go(gl=gl, h=h):
                for k in range(2):
                    copy(gl, h, k).start()

            def keep(gl=gl, h=h):
                got_ref[dp] = main_ref[gl, h]
                gint_ref[dp] = ints_ref[gl, h]

            pl.when(jnp.logical_not(is_own(gl, h)))(go)
            pl.when(is_own(gl, h))(keep)
    for q in range(4):

        def take(q=q):
            for k, d in enumerate((got_ref, gint_ref)):
                pltpu.make_async_remote_copy(
                    src_ref=d.at[q],
                    dst_ref=d.at[q],
                    send_sem=send_sems.at[k],
                    recv_sem=recv_sems.at[q, k],
                    device_id={"dp": jnp.int32(q), "tp": tp},
                    device_id_type=MESH,
                ).wait_recv()

        pl.when(jnp.logical_not(jnp.logical_and(q == dp, dp // 2 == tp)))(take)
    for gl in range(2):
        for h in range(2):

            def done(gl=gl, h=h):
                for k in range(2):
                    copy(gl, h, k).wait_send()

            pl.when(jnp.logical_not(is_own(gl, h)))(done)


def spread(main, ints):
    return pl.pallas_call(
        spread_kernel,
        out_shape=[
            jax.ShapeDtypeStruct((4,) + main.shape[2:], main.dtype),
            jax.ShapeDtypeStruct((4,) + ints.shape[2:], ints.dtype),
        ],
        in_specs=[pl.BlockSpec(memory_space=VMEM)] * 2,
        out_specs=[pl.BlockSpec(memory_space=VMEM)] * 2,
        scratch_shapes=[pltpu.SemaphoreType.DMA((8,)), pltpu.SemaphoreType.DMA((4, 2))],
        compiler_params=pltpu.CompilerParams(
            collective_id=1, has_side_effects=True, vmem_limit_bytes=16 << 20
        ),
        name="spread",
    )(main, ints)


def bases(spans):
    return [sum(spans[:r]) for r in range(4)]


def kv_kernel(spans, order_ref, got_ref, w_ref, out_ref, wo_ref, own, send_sems, recv_sems):
    z, y = place()
    tp, dp = lax.axis_index("tp"), lax.axis_index("dp")
    pair = {"tp": 1 - tp}
    base = bases(spans)
    for r, rows in enumerate(spans):

        def fill(r=r):
            piece = got_ref[order_ref[r], :, pl.ds(PER * HEAD, 2 * HEAD)]
            own[r] = piece
            out_ref[tp, base[r] + z, y] = piece

        when(True if rows == N else z < rows, fill)
    left, right = lax.rem(dp + 3, 4), lax.rem(dp + 1, 4)
    barrier(plane_partners(z, y) + [pair, {"dp": left}, {"dp": right}])
    c = Copies(send_sems, recv_sems)
    mine = w_ref
    xs = []
    for to in (right, left):
        i = c.slot()
        c.send(i, mine, wo_ref.at[tp, dp], {"dp": to})
        xs.append((i, mine, {"dp": to}))
    i_own = c.slot()
    c.send(i_own, mine, wo_ref.at[tp, dp], pair)
    local = pltpu.make_async_copy(mine, wo_ref.at[tp, dp], send_sems.at[c.slot()])
    local.start()

    jobs = []
    for r, rows in enumerate(spans):

        split = SPLIT if r == 0 else 0

        def part_rows(part, split=split):
            return pl.ds(0, split) if part == 0 else pl.ds(split, ROWS - split)

        def src(part, r=r, part_rows=part_rows):
            return own.at[r, part_rows(part)]

        def view(z0, nz, y0, ny, part, r=r, part_rows=part_rows):
            zi = base[r] + z0 if nz == 1 else pl.ds(base[r] + z0, nz)
            yi = y0 if ny == 1 else pl.ds(y0, ny)
            return out_ref.at[tp, zi, yi, part_rows(part)]

        jobs.append(Gather(c, src, view, rows, True, pair, (r == 0, True), r % 2 == 1))
    for g in jobs:
        g.first()
    mirrors = []
    seconds = []
    for k in range(1, 6):
        for g in jobs:
            for step in g.hop(k):
                step()
        if k == 3:
            for n, (frm, to, half) in enumerate(((left, right, 0), (right, left, 1))):
                i = xs[n][0]
                ref = wo_ref.at[tp, frm]
                c.arrived(i, ref, {"dp": to})
                part = wo_ref.at[tp, frm, pl.ds(half * 4, 4)]
                i2 = c.slot()
                c.send(i2, part, part, {"dp": to})
                seconds.append((i2, part, {"dp": to}, half))
                i3 = c.slot()
                c.send(i3, ref, ref, pair)
                mirrors.append((i3, ref))
    far = lax.rem(dp + 2, 4)
    for i2, part, to, half in seconds:
        ref = wo_ref.at[tp, far, pl.ds(half * 4, 4)]
        c.arrived(i2, ref, to)
        i3 = c.slot()
        c.send(i3, ref, ref, pair)
        mirrors.append((i3, ref))
    assert c.used <= send_sems.shape[0], c.used
    for g in jobs:
        g.last()
    c.arrived(i_own, wo_ref.at[tp, dp], pair)
    c.left(i_own, mine, pair)
    for i, ref in mirrors:
        c.arrived(i, ref, pair)
        c.left(i, ref, pair)
    for i, ref, to in xs:
        c.left(i, ref, to)
    for i2, part, to, half in seconds:
        c.left(i2, part, to)
    local.wait()


def gather_kv(order, got, w_part, spans, number, limit):
    vm = pl.BlockSpec(memory_space=VMEM)
    return pl.pallas_call(
        functools.partial(kv_kernel, spans),
        out_shape=[
            jax.ShapeDtypeStruct((2, sum(spans), N, ROWS, 2 * HEAD), got.dtype),
            jax.ShapeDtypeStruct((2, 4, N, N, 32, 128), got.dtype),
        ],
        in_specs=[pl.BlockSpec(memory_space=SMEM), vm, pl.BlockSpec(memory_space=HBM)],
        out_specs=[vm, vm],
        scratch_shapes=[
            pltpu.VMEM((4, ROWS, 2 * HEAD), jnp.bfloat16),
            pltpu.SemaphoreType.DMA((limit,)),
            pltpu.SemaphoreType.DMA((limit,)),
        ],
        compiler_params=pltpu.CompilerParams(
            collective_id=number,
            has_side_effects=True,
            vmem_limit_bytes=(24 if sum(spans) < 20 else 56) << 20,
        ),
        name="gather_kv",
    )(order, got, w_part)


def attend_kernel(spans, order_ref, ints_ref, main_ref, kv_ref, block_ref, out_ref, buf, comp, gates):
    kv, tp = lax.axis_index("kv"), lax.axis_index("tp")
    start = kv * (2 * HALF) + tp * HALF
    base = bases(spans)
    lane = lax.broadcasted_iota(jnp.int32, (BLK, 128), 1)
    row_in = lax.rem(lax.broadcasted_iota(jnp.int32, (PER * BLK, 1), 0), BLK)
    comp[...] = jnp.zeros_like(comp)
    to_row = lax.broadcasted_iota(jnp.int32, (48, 256), 0)
    from_row = lax.broadcasted_iota(jnp.int32, (48, 256), 1)
    piece = (to_row * 21846) >> 16
    pick_rows = jnp.where(from_row == piece * 16 + (to_row - piece * 3), 1.0, 0.0).astype(jnp.bfloat16)
    turn = jnp.where(
        lax.rem(lax.broadcasted_iota(jnp.int32, (16, 128), 0), 8)
        == lax.broadcasted_iota(jnp.int32, (16, 128), 1),
        1.0,
        0.0,
    ).astype(jnp.bfloat16)
    block_ends = block_ref[...] * BLK + (BLK - 1)

    def step(n, carry):
        r = (n * 21846) >> 16
        j = n - r * 3
        seq = order_ref[r]
        rows = pl.ds(pl.multiple_of(j * BLK, BLK), BLK)
        live = start < ints_ref[seq, 7, 0]
        first = jnp.int32(base[0])
        for q in range(1, 4):
            first = jnp.where(r == q, base[q], first)

        @pl.when(jnp.logical_and(live, j == 0))
        def _():
            def pack(z, carry):
                tile = kv_ref[:, first + z, :, pl.ds(HALF, 16), :].reshape(256, 128)
                got = jnp.dot(pick_rows, tile, preferred_element_type=jnp.float32)
                comp[pl.ds(pl.multiple_of(z * 48, 16), 48), :] = got.astype(jnp.bfloat16)
                return carry

            lax.fori_loop(0, kv // N + 1, pack, 0)
            gates[...] = lax.dot_general(
                main_ref[seq, pl.ds(HALF, 16), pl.ds(0, HALF + 64)],
                turn,
                (((0,), (0,)), ((), ())),
                preferred_element_type=jnp.float32,
            )

        @pl.when(jnp.logical_not(live))
        def _():
            out_ref[seq, rows] = jnp.zeros((BLK, PER * HEAD), jnp.bfloat16)

        @pl.when(live)
        def _():
            def fetch(p, count):
                b = ints_ref[seq, j, p]

                @pl.when(b >= 0)
                def _():
                    span = (b * 10923) >> 16
                    at = b - span * 6
                    t = jnp.where(at >= 3, 1, 0)
                    row = (at - t * 3) * BLK
                    buf[pl.ds(pl.multiple_of(count * BLK, BLK), BLK), :] = kv_ref[
                        t,
                        first + (span >> 3),
                        span & 7,
                        pl.ds(pl.multiple_of(row, BLK), BLK),
                        :,
                    ]

                return count + jnp.where(b >= 0, 1, 0)

            count = lax.fori_loop(0, PICKS, fetch, jnp.int32(0), unroll=True)
            parts = []
            for h in range(PER):
                two = main_ref[seq, rows, pl.ds((h // 2) * 128, 128)].astype(jnp.float32) * 0.125
                if h % 2:
                    two = pltpu.roll(two, 64, 1)
                parts.append(jnp.where(lane < HEAD, two, 0.0).astype(jnp.bfloat16))
            q = jnp.concatenate(parts, axis=0)

            def score(keys):
                return lax.dot_general(
                    q, keys, (((1,), (1,)), ((), ())), preferred_element_type=jnp.float32
                )

            spot = start + j * BLK + row_in
            keys = comp[...]
            seen = block_ends <= spot
            cs = jnp.where(seen, score(keys), MASKED)
            ctop = jnp.max(cs, axis=-1, keepdims=True)
            cw = jnp.exp(cs - ctop)
            cn = jnp.maximum(jnp.sum(cw, axis=-1, keepdims=True), 1.0)
            cp = (cw * jnp.where(spot >= BLK - 1, 1.0 / cn, 0.0)).astype(jnp.bfloat16)
            co = jnp.dot(cp, keys, preferred_element_type=jnp.float32)

            own = main_ref[seq, rows, pl.ds(PER * HEAD, 128)]
            ks = lax.broadcasted_iota(jnp.int32, (1, BLK), 1)

            def finish(so):
                mixed = []
                g = gates[pl.ds(pl.multiple_of(j * BLK, BLK), BLK), :]
                for h in range(PER):
                    at = slice(h * BLK, (h + 1) * BLK)
                    mixed.append(g[:, h : h + 1] * co[at] + g[:, 4 + h : 5 + h] * so[at])
                for h in range(2):
                    pair = jnp.where(
                        lane < HEAD, pltpu.roll(mixed[2 * h], 64, 1), mixed[2 * h + 1]
                    )
                    out_ref[seq, rows, pl.ds(h * 128, 128)] = pair.astype(jnp.bfloat16)

            def own_scores():
                return jnp.where(ks <= row_in, score(own), MASKED)

            @pl.when(count == 0)
            def _():
                os = own_scores()
                ow = jnp.exp(os - jnp.max(os, axis=-1, keepdims=True))
                inv = 1.0 / jnp.sum(ow, axis=-1, keepdims=True)
                finish(jnp.dot((ow * inv).astype(jnp.bfloat16), own, preferred_element_type=jnp.float32))

            @pl.when(count > 0)
            def _():
                os = own_scores()
                far = buf[...]
                spots = lax.broadcasted_iota(jnp.int32, (1, PICKS * BLK), 1)
                fs = jnp.where(spots < count * BLK, score(far), MASKED)
                top = jnp.maximum(
                    jnp.max(os, axis=-1, keepdims=True), jnp.max(fs, axis=-1, keepdims=True)
                )
                ow, fw = jnp.exp(os - top), jnp.exp(fs - top)
                inv = 1.0 / (
                    jnp.sum(ow, axis=-1, keepdims=True) + jnp.sum(fw, axis=-1, keepdims=True)
                )
                so = jnp.dot(
                    (ow * inv).astype(jnp.bfloat16), own, preferred_element_type=jnp.float32
                ) + jnp.dot((fw * inv).astype(jnp.bfloat16), far, preferred_element_type=jnp.float32)
                finish(so)

        return carry

    buf[...] = jnp.zeros_like(buf)
    lax.fori_loop(0, 12, step, 0)


def attend(spans, order, gint, got, gathered):
    vm = pl.BlockSpec(memory_space=VMEM)
    sm = pl.BlockSpec(memory_space=SMEM)
    c = jnp.arange(384, dtype=jnp.int32)
    z, t, y, j = c // 48, c % 48 // 24, c % 24 // 3, c % 3
    blocks = ((z * N + y) * 6 + t * 3 + j)[None]
    return pl.pallas_call(
        functools.partial(attend_kernel, spans),
        out_shape=jax.ShapeDtypeStruct((4, HALF, PER * HEAD), jnp.bfloat16),
        in_specs=[sm, sm, vm, vm, vm],
        out_specs=vm,
        scratch_shapes=[
            pltpu.VMEM((PICKS * BLK, 2 * HEAD), jnp.bfloat16),
            pltpu.VMEM((384, 2 * HEAD), jnp.bfloat16),
            pltpu.VMEM((HALF + 64, 128), jnp.float32),
        ],
        compiler_params=pltpu.CompilerParams(vmem_limit_bytes=(24 if sum(spans) < 20 else 48) << 20),
        name="attend",
    )(order, gint, got, gathered, blocks)


def finish_kernel(len_ref, att_ref, wo_ref, out_ref, back, send_sems, recv_sems):
    dp, kv, tp = lax.axis_index("dp"), lax.axis_index("kv"), lax.axis_index("tp")
    barrier([{"dp": lax.rem(dp + d, 4)} for d in range(1, 4)])

    def copy(d):
        to = lax.rem(dp + d, 4)
        return pltpu.make_async_remote_copy(
            src_ref=att_ref.at[to],
            dst_ref=back.at[dp],
            send_sem=send_sems.at[d],
            recv_sem=recv_sems.at[d],
            device_id={"dp": to},
            device_id_type=MESH,
        )

    for d in (2, 1, 3):
        copy(d).start()
    back[dp] = att_ref[dp]
    for d in (1, 3, 2):
        frm = lax.rem(dp + 4 - d, 4)
        pltpu.make_async_remote_copy(
            src_ref=back.at[frm],
            dst_ref=back.at[frm],
            send_sem=send_sems.at[d],
            recv_sem=recv_sems.at[d],
            device_id={"dp": frm},
            device_id_type=MESH,
        ).wait_recv()
    spot = kv * (2 * HALF) + tp * HALF + lax.broadcasted_iota(jnp.int32, (HALF, 1), 0)
    alive = spot < len_ref[0]
    cols = [jnp.concatenate([back[2 * t], back[2 * t + 1]], axis=1) for t in range(2)]

    def tile(z, carry):
        total = jnp.zeros((HALF, 256), jnp.float32)
        for t in range(2):
            w = jnp.concatenate([wo_ref[t, q, z].reshape(256, 128) for q in range(4)], axis=1)
            part = lax.dot_general(
                cols[t], w, (((1,), (1,)), ((), ())), preferred_element_type=jnp.float32
            )
            total = total + part.astype(jnp.bfloat16).astype(jnp.float32)
        out_ref[:, pl.ds(pl.multiple_of(z * 256, 256), 256)] = jnp.where(alive, total, 0.0).astype(
            jnp.bfloat16
        )
        return carry

    lax.fori_loop(0, N, tile, 0)
    for d in (1, 2, 3):
        copy(d).wait_send()


def finish(length, att, wo, number):
    vm = pl.BlockSpec(memory_space=VMEM)
    return pl.pallas_call(
        finish_kernel,
        out_shape=jax.ShapeDtypeStruct((HALF, 2048), jnp.bfloat16),
        in_specs=[pl.BlockSpec(memory_space=SMEM), vm, vm],
        out_specs=vm,
        scratch_shapes=[
            pltpu.VMEM((4, HALF, PER * HEAD), jnp.bfloat16),
            pltpu.SemaphoreType.DMA((4,)),
            pltpu.SemaphoreType.DMA((4,)),
        ],
        compiler_params=pltpu.CompilerParams(
            collective_id=number, has_side_effects=True, vmem_limit_bytes=24 << 20
        ),
        name="finish",
    )(length, att, wo)


def by_halves(a):
    return a.reshape(2, HALF, *a.shape[1:])


def body(
    tokens, seq_lengths, block_picks, w_query, w_key, w_value, w_gate, w_ckey, w_cvalue, w_out
):
    x = tokens[0]
    kv, tp, dp = lax.axis_index("kv"), lax.axis_index("tp"), lax.axis_index("dp")
    out_part = lax.dynamic_slice_in_dim(w_out.T, dp * 128, 128, axis=1)
    piece = jnp.concatenate(
        [
            w_query[:, :256],
            w_key[:, :64],
            w_value[:, :64],
            w_query[:, 256:],
            w_key[:, 64:],
            w_value[:, 64:],
        ],
        axis=1,
    )
    w_all, w_part = gather_weights(piece, out_part)

    gate_all = jax.nn.sigmoid(jnp.dot(x, w_gate, preferred_element_type=jnp.float32))
    gate_all = gate_all.reshape(384, 2, 2, 2, PER)
    gate_own = lax.dynamic_index_in_dim(gate_all, tp, 2, keepdims=False)
    gate_own = gate_own.transpose(2, 1, 3, 0).reshape(2, 8, 2, HALF).transpose(0, 2, 1, 3)
    hi = gate_own.astype(jnp.bfloat16)
    lo = (gate_own - hi.astype(jnp.float32)).astype(jnp.bfloat16)
    gate_rows = jnp.concatenate([hi, lo], axis=2)
    gate_rows = jnp.pad(gate_rows, ((0, 0), (0, 0), (0, 0), (0, 64)))

    qkv = jnp.dot(x, w_all.reshape(2048, 768), preferred_element_type=jnp.float32).astype(jnp.bfloat16)
    mains = []
    for gl in range(2):
        one = qkv[:, gl * 384 : (gl + 1) * 384]
        ck = jnp.dot(
            one[:, 256:320].reshape(6, BLK * HEAD), w_ckey, preferred_element_type=jnp.float32
        )
        cv = jnp.dot(
            one[:, 320:384].reshape(6, BLK * HEAD), w_cvalue, preferred_element_type=jnp.float32
        )
        pairs = jnp.concatenate([ck, cv], axis=1).astype(jnp.bfloat16).reshape(2, 3, 128)
        pairs = jnp.pad(pairs, ((0, 0), (0, 13), (0, 0)))
        extra = jnp.concatenate([gate_rows[gl], pairs], axis=2)
        mains.append(jnp.concatenate([by_halves(one), extra], axis=1))
    main = jnp.stack(mains)

    picks = block_picks[0].transpose(1, 0, 2).reshape(2, 2, 3, PICKS)
    ints = jnp.pad(picks, ((0, 0), (0, 0), (0, 5), (0, 112)))
    row = lax.broadcasted_iota(jnp.int32, ints.shape, 2)
    ints = jnp.where(row == 7, seq_lengths[0], ints)

    got, gint = spread(main, ints)
    lens = gint[:, 7, 0]
    ids = jnp.arange(4, dtype=jnp.int32)
    ahead = (lens[None, :] > lens[:, None]) | (
        (lens[None, :] == lens[:, None]) & (ids[None, :] < ids[:, None])
    )
    rank = jnp.sum(ahead.astype(jnp.int32), axis=1)
    order = jnp.sum(jnp.where(rank[None, :] == ids[:, None], ids[None, :], 0), axis=1)
    ranked = jnp.sum(
        jnp.where(rank[None, :] == ids[:, None], lens[None, :], 0), axis=1
    )

    def run(spans, number, limit):
        gathered, wo = gather_kv(order, got, w_part, spans, number, limit)
        att = attend(spans, order, gint, got, gathered)
        return finish(seq_lengths, att, wo, number + 1)

    span = N * 384
    small = (ranked[1] <= 3 * span) & (ranked[2] <= 2 * span) & (ranked[3] <= span)
    out = lax.cond(
        small, lambda: run((8, 3, 2, 1), 2, 448), lambda: run((8, 8, 8, 8), 4, 600)
    )
    return out[None]


def solution(mesh):
    return jax.shard_map(
        body,
        mesh=mesh,
        in_specs=(
            P("dp", "kv", None),
            P("dp"),
            P("dp", "kv", "tp", None),
            P("kv", "tp"),
            P("kv", "tp"),
            P("kv", "tp"),
            P(),
            P(),
            P(),
            P("tp", "kv"),
        ),
        out_specs=P("dp", ("kv", "tp"), None),
        check_vma=False,
    )
```

```python
import functools

import jax
import jax.numpy as jnp
from jax import lax
from jax.experimental import pallas as pl
from jax.experimental.pallas import tpu as pltpu
from jax.sharding import PartitionSpec as P

MESH = pl.DeviceIdType.MESH

HEADS = 16
GROUPS = 4
PER = 4
HEAD = 64
BLK = 64
PICKS = 16
N = 8
ROWS = 208
HALF = 192
SPLIT = 112
MASKED = -1e30
VMEM = pltpu.MemorySpace.VMEM
SMEM = pltpu.MemorySpace.SMEM
HBM = pltpu.MemorySpace.HBM


def place():
    kv = lax.axis_index("kv")
    return kv // N, lax.rem(kv, N)


class Copies:
    def __init__(self, send_sems, recv_sems):
        self.send_sems, self.recv_sems, self.used, self.sent = send_sems, recv_sems, 0, []

    def slot(self):
        self.used += 1
        return self.used - 1

    def send(self, i, src, dst, device):
        copy = pltpu.make_async_remote_copy(
            src_ref=src,
            dst_ref=dst,
            send_sem=self.send_sems.at[i],
            recv_sem=self.recv_sems.at[i],
            device_id=device,
            device_id_type=MESH,
        )
        copy.start()

    def arrived(self, i, ref, device):
        pltpu.make_async_remote_copy(
            src_ref=ref,
            dst_ref=ref,
            send_sem=self.send_sems.at[i],
            recv_sem=self.recv_sems.at[i],
            device_id=device,
            device_id_type=MESH,
        ).wait_recv()

    def left(self, i, ref, device):
        pltpu.make_async_remote_copy(
            src_ref=ref,
            dst_ref=ref,
            send_sem=self.send_sems.at[i],
            recv_sem=self.recv_sems.at[i],
            device_id=device,
            device_id_type=MESH,
        ).wait_send()


def when(cond, fn):
    if cond is True:
        fn()
    elif cond is not False:
        pl.when(cond)(fn)


def both(a, b):
    if a is True:
        return b
    if b is True:
        return a
    if a is False or b is False:
        return False
    return jnp.logical_and(a, b)


def wrap(i):
    return lax.rem(i + N, N)


def barrier(kinds):
    sem = pltpu.get_barrier_semaphore()
    for device in kinds:
        pl.semaphore_signal(sem, inc=1, device_id=device, device_id_type=MESH)
    pl.semaphore_wait(sem, len(kinds))


def plane_partners(z, y):
    return [{"kv": z * N + wrap(y + d)} for d in range(1, N)] + [
        {"kv": wrap(z + d) * N + y} for d in range(1, N)
    ]


class Gather:
    def __init__(
        self, copies, src, view, rows, causal, pair, parts=(True, True), tie=False, only=True
    ):
        self.c, self.src, self.view, self.rows, self.causal = copies, src, view, rows, causal
        self.pair, self.parts, self.tie = pair, parts, tie
        self.z, self.y = place()
        self.live = True if rows == N else self.z < rows
        self.only = only
        self.waits = []
        self.pair_waits = []
        self.flight = {}
        if not causal:
            self.subs_b = [(0, 4), (4, 4)]
        elif rows == N:
            self.subs_b = [(0, 1), (1, 1), (2, 2), (4, 2), (6, 2)]
        else:
            self.subs_b = [(i, 1) for i in range(rows)]

    def dev(self, z, y):
        return {"kv": z * N + y}

    def transfer(self, cond_send, src, dst, device, cond_recv, got):
        i = self.c.slot()
        cond_send, cond_recv = both(cond_send, self.only), both(cond_recv, self.only)
        when(cond_send, lambda: self.c.send(i, src, dst, device))
        self.waits.append((i, cond_send, src, device))
        return (i, cond_recv, got, device)

    def take(self, t):
        i, cond, ref, device = t
        when(cond, lambda: self.c.arrived(i, ref, device))

    def mirror(self, cond, ref):
        if self.pair is None:
            return
        i = self.c.slot()
        send, recv = cond, cond
        if self.only is not True:
            send, recv = self.only, jnp.logical_not(self.only)
        when(send, lambda: self.c.send(i, ref, ref, self.pair))
        self.pair_waits.append((i, send, recv, ref))

    def first(self):
        z, y = self.z, self.y
        self.a1, self.b1 = [], []
        for d in range(1, N) if self.parts[0] else ():
            self.a1.append(
                self.transfer(
                    self.live,
                    self.src(0),
                    self.view(z, 1, y, 1, 0),
                    self.dev(z, wrap(y + d)),
                    self.live,
                    self.view(z, 1, wrap(y - d), 1, 0),
                )
            )
        reach = N if not self.causal else self.rows
        for d in range(1, reach) if self.parts[1] else ():
            cs = True if not self.causal else z + d < self.rows
            cr = True if not self.causal else both(self.live, z - d >= 0)
            self.b1.append(
                self.transfer(
                    cs,
                    self.src(1),
                    self.view(z, 1, y, 1, 1),
                    self.dev(wrap(z + d), y),
                    cr,
                    self.view(wrap(z - d), 1, y, 1, 1),
                )
            )

    def ring_y(self, k, z0, nz, part, right, cond):
        z, y = self.z, self.y
        if right:
            o, got, to = wrap(y - (k - 1)), wrap(y - k), wrap(y + 1)
        else:
            o, got, to = lax.rem(y + k - 1, N), lax.rem(y + k, N), wrap(y - 1)
        return self.transfer(
            cond,
            self.view(z0, nz, o, 1, part),
            self.view(z0, nz, o, 1, part),
            self.dev(z, to),
            cond,
            self.view(z0, nz, got, 1, part),
        )

    def hop_a(self, right, sub, k, depth):
        z, y = self.z, self.y
        y0, ny = (sub * 4, 4)
        if right:
            o, got, to = wrap(z - (k - 1)), wrap(z - k), wrap(z + 1)
            cs = both(z - (k - 1) >= 0, z + 1 < self.rows) if self.causal else True
            cr = both(self.live, z - k >= 0) if self.causal else True
        else:
            o, got, to = wrap(z + k - 1), lax.rem(z + k, N), wrap(z - 1)
            cs = o < depth if self.causal else True
            cr = got < depth if self.causal else True
        return self.transfer(
            cs,
            self.view(o, 1, y0, ny, 0),
            self.view(o, 1, y0, ny, 0),
            self.dev(to, y),
            cr,
            self.view(got, 1, y0, ny, 0),
        )

    def hop_b(self, right, sub, k):
        z0, nz = self.subs_b[sub]
        cond = self.live
        if self.causal and z0 > 0:
            cond = both(cond, self.z >= z0)
        return self.ring_y(k, z0, nz, 1, right, cond)

    def depth_a(self, right, sub):
        if self.rows < N:
            return self.rows - 1 if right else 0
        return 4 if right == (sub == 0) else 3

    def depth_b(self, right, sub):
        return 4 if right == ((sub % 2 == 0) != self.tie) else 3

    def hop(self, k):
        steps = []
        order = [("a", 0), ("b", 0), ("b", 1), ("a", 1)] + [("b", i) for i in range(2, 5)]
        begun = set()
        for ring, s in order:
            if s >= (2 if ring == "a" else len(self.subs_b)) or not self.parts[ring == "b"]:
                continue
            if k == 1 and ring not in begun:
                begun.add(ring)
                steps.append(lambda ring=ring: self.begin(ring))
            for r in (True, False):
                steps.append(lambda ring=ring, s=s, r=r: self.lane(ring, s, r, k))
        return steps

    def begin(self, ring):
        for t in self.a1 if ring == "a" else self.b1:
            self.take(t)

    def lane(self, ring, s, r, k):
        depth = self.depth_a(r, s) if ring == "a" else self.depth_b(r, s)
        got = None
        if 1 < k <= depth + 1:
            got = self.flight[ring, r, s]
            self.take(got)
        if k <= depth:
            self.flight[ring, r, s] = (
                self.hop_a(r, s, k, depth) if ring == "a" else self.hop_b(r, s, k)
            )
        if got is not None:
            self.mirror(got[1], got[2])
        if k == 1 and r:
            if ring == "a":
                self.mirror(self.live, self.view(self.z, 1, s * 4, 4, 0))
            else:
                z0, nz = self.subs_b[s]
                cond = both(self.live, self.z >= z0) if z0 and self.causal else self.live
                self.mirror(cond, self.view(z0, nz, self.y, 1, 1))

    def last(self):
        for i, send, recv, ref in self.pair_waits:
            when(recv, lambda: self.c.arrived(i, ref, self.pair))
            when(send, lambda: self.c.left(i, ref, self.pair))
        for i, cond, ref, device in self.waits:
            when(cond, lambda: self.c.left(i, ref, device))


def spread_partners(dp, tp):
    return [{"dp": lax.rem(dp + e // 2, 4), "tp": lax.rem(tp + e % 2, 2)} for e in range(1, 8)]


def entry_kernel(
    x_ref, w_ref, o_ref, ints_ref, tok_ref, wall_ref, wo_ref, gint_ref, send_sems, recv_sems, int_sems, local_sem
):
    z, y = place()
    dp, tp = lax.axis_index("dp"), lax.axis_index("tp")
    pair = {"tp": 1 - tp}
    owner = dp // 2 == tp
    mine = x_ref.at[pl.ds(pl.multiple_of(tp * HALF, HALF), HALF)]
    local = pltpu.make_async_copy(mine, tok_ref.at[dp], local_sem)
    local.start()
    wo_ref[tp, z, y] = o_ref[...]

    @pl.when(owner)
    def _():
        wall_ref[z, y] = w_ref[...]

    barrier(plane_partners(z, y) + spread_partners(dp, tp))
    c = Copies(send_sems, recv_sems)

    left, right = lax.rem(dp + 3, 4), lax.rem(dp + 1, 4)
    part = HALF // 2
    first = {}
    for way, to, subs in (("r", right, (0, 1)), ("l", left, (1, 0))):
        for sub in subs:
            i = c.slot()
            src = x_ref.at[pl.ds(pl.multiple_of(tp * HALF + sub * part, part), part)]
            c.send(i, src, tok_ref.at[dp, pl.ds(sub * part, part)], {"dp": to})
            first[way, sub] = (i, src, to)

    def int_copy(gl, h):
        return pltpu.make_async_remote_copy(
            src_ref=ints_ref.at[gl, h],
            dst_ref=gint_ref.at[dp],
            send_sem=int_sems.at[gl * 2 + h],
            recv_sem=int_sems.at[4 + dp],
            device_id={"dp": 2 * tp + gl, "tp": jnp.int32(h)},
            device_id_type=MESH,
        )

    def is_own(gl, h):
        return jnp.logical_and(2 * tp + gl == dp, tp == h)

    for gl in range(2):
        for h in range(2):

            def go(gl=gl, h=h):
                int_copy(gl, h).start()

            def keep(gl=gl, h=h):
                gint_ref[dp] = ints_ref[gl, h]

            pl.when(jnp.logical_not(is_own(gl, h)))(go)
            pl.when(is_own(gl, h))(keep)

    jobs = []
    for src_ref, out_ref, only in ((o_ref, wo_ref.at[tp], True), (w_ref, wall_ref, owner)):
        half = src_ref.shape[0] // 2

        def src(part, src_ref=src_ref, half=half):
            return src_ref.at[pl.ds(part * half, half)]

        def view(z0, nz, y0, ny, part, out_ref=out_ref, half=half):
            zi = z0 if nz == 1 else pl.ds(z0, nz)
            yi = y0 if ny == 1 else pl.ds(y0, ny)
            return out_ref.at[zi, yi, pl.ds(part * half, half)]

        jobs.append(Gather(c, src, view, N, False, pair, only=only))
    for g in jobs:
        g.first()
    second = []

    def onward(way, sub, frm, to):
        i = first[way, sub][0]
        ref = tok_ref.at[frm, pl.ds(sub * part, part)]
        c.arrived(i, ref, {"dp": to})
        i2 = c.slot()
        c.send(i2, ref, ref, {"dp": to})
        second.append((i2, ref, sub, to))

    for k in range(1, 6):
        for g in jobs:
            for step in g.hop(k):
                step()
        if k == 2:
            onward("r", 0, left, right)
            onward("l", 1, right, left)
    assert c.used <= send_sems.shape[0], c.used
    for g in jobs:
        g.last()
    for q in range(4):

        def take(q=q):
            ref = gint_ref.at[q]
            pltpu.make_async_remote_copy(
                src_ref=ref,
                dst_ref=ref,
                send_sem=int_sems.at[0],
                recv_sem=int_sems.at[4 + q],
                device_id={"dp": jnp.int32(q), "tp": tp},
                device_id_type=MESH,
            ).wait_recv()

        pl.when(jnp.logical_not(jnp.logical_and(q == dp, owner)))(take)
    for gl in range(2):
        for h in range(2):
            pl.when(jnp.logical_not(is_own(gl, h)))(lambda gl=gl, h=h: int_copy(gl, h).wait_send())
    local.wait()
    for way, sub, frm, to in (("r", 1, left, right), ("l", 0, right, left)):
        c.arrived(first[way, sub][0], tok_ref.at[frm, pl.ds(sub * part, part)], {"dp": to})
    far = lax.rem(dp + 2, 4)
    for i2, ref, sub, to in second:
        c.arrived(i2, tok_ref.at[far, pl.ds(sub * part, part)], {"dp": to})
    for i, src, to in first.values():
        c.left(i, src, {"dp": to})
    for i2, ref, sub, to in second:
        c.left(i2, ref, {"dp": to})


def entry(x, w, o, ints):
    vm = pl.BlockSpec(memory_space=VMEM)
    return pl.pallas_call(
        entry_kernel,
        out_shape=[
            jax.ShapeDtypeStruct((4, HALF, x.shape[1]), x.dtype),
            jax.ShapeDtypeStruct((N, N) + w.shape, w.dtype),
            jax.ShapeDtypeStruct((2, N, N) + o.shape, o.dtype),
            jax.ShapeDtypeStruct((4,) + ints.shape[2:], ints.dtype),
        ],
        in_specs=[pl.BlockSpec(memory_space=HBM), vm, vm, vm],
        out_specs=[vm] * 4,
        scratch_shapes=[
            pltpu.SemaphoreType.DMA((192,)),
            pltpu.SemaphoreType.DMA((192,)),
            pltpu.SemaphoreType.DMA((8,)),
            pltpu.SemaphoreType.DMA,
        ],
        compiler_params=pltpu.CompilerParams(
            collective_id=0, has_side_effects=True, vmem_limit_bytes=24 << 20
        ),
        name="entry",
    )(x, w, o, ints)


def bases(spans):
    return [sum(spans[:r]) for r in range(4)]


def kv_kernel(spans, order_ref, got_ref, pairs_ref, out_ref, own, send_sems, recv_sems):
    z, y = place()
    tp = lax.axis_index("tp")
    pair = {"tp": 1 - tp}
    base = bases(spans)
    for r, rows in enumerate(spans):

        def fill(r=r):
            seq = order_ref[r]
            piece = got_ref[seq, :, pl.ds(PER * HEAD, 2 * HEAD)]
            pairs = pairs_ref[seq]
            for ref in (own.at[r], out_ref.at[tp, base[r] + z, y]):
                ref[pl.ds(0, HALF)] = piece
                ref[pl.ds(HALF, ROWS - HALF)] = pairs

        when(True if rows == N else z < rows, fill)
    barrier(plane_partners(z, y) + [pair])
    c = Copies(send_sems, recv_sems)
    jobs = []
    for r, rows in enumerate(spans):

        split = SPLIT if r == 0 else 0

        def part_rows(part, split=split):
            return pl.ds(0, split) if part == 0 else pl.ds(split, ROWS - split)

        def src(part, r=r, part_rows=part_rows):
            return own.at[r, part_rows(part)]

        def view(z0, nz, y0, ny, part, r=r, part_rows=part_rows):
            zi = base[r] + z0 if nz == 1 else pl.ds(base[r] + z0, nz)
            yi = y0 if ny == 1 else pl.ds(y0, ny)
            return out_ref.at[tp, zi, yi, part_rows(part)]

        jobs.append(Gather(c, src, view, rows, True, pair, (r == 0, True), r % 2 == 1))
    for g in jobs:
        g.first()
    for k in range(1, 6):
        for g in jobs:
            for step in g.hop(k):
                step()
    assert c.used <= send_sems.shape[0], c.used
    for g in jobs:
        g.last()


def gather_kv(order, got, pairs, spans, number, limit):
    vm = pl.BlockSpec(memory_space=VMEM)
    return pl.pallas_call(
        functools.partial(kv_kernel, spans),
        out_shape=jax.ShapeDtypeStruct((2, sum(spans), N, ROWS, 2 * HEAD), got.dtype),
        in_specs=[pl.BlockSpec(memory_space=SMEM), vm, vm],
        out_specs=vm,
        scratch_shapes=[
            pltpu.VMEM((4, ROWS, 2 * HEAD), jnp.bfloat16),
            pltpu.SemaphoreType.DMA((limit,)),
            pltpu.SemaphoreType.DMA((limit,)),
        ],
        compiler_params=pltpu.CompilerParams(
            collective_id=number,
            has_side_effects=True,
            vmem_limit_bytes=(24 if sum(spans) < 20 else 40) << 20,
        ),
        name="gather_kv",
    )(order, got, pairs)


def attend_kernel(
    spans, order_ref, ints_ref, main_ref, gate_ref, kv_ref, block_ref, out_ref, buf, comp
):
    kv, tp = lax.axis_index("kv"), lax.axis_index("tp")
    start = kv * (2 * HALF) + tp * HALF
    base = bases(spans)
    lane = lax.broadcasted_iota(jnp.int32, (BLK, 128), 1)
    row_in = lax.rem(lax.broadcasted_iota(jnp.int32, (PER * BLK, 1), 0), BLK)
    comp[...] = jnp.zeros_like(comp)
    to_row = lax.broadcasted_iota(jnp.int32, (48, 256), 0)
    from_row = lax.broadcasted_iota(jnp.int32, (48, 256), 1)
    piece = (to_row * 21846) >> 16
    pick_rows = jnp.where(from_row == piece * 16 + (to_row - piece * 3), 1.0, 0.0).astype(jnp.bfloat16)
    block_ends = block_ref[...] * BLK + (BLK - 1)

    def step(n, carry):
        r = (n * 21846) >> 16
        j = n - r * 3
        seq = order_ref[r]
        rows = pl.ds(pl.multiple_of(j * BLK, BLK), BLK)
        live = start < ints_ref[seq, 7, 0]
        first = jnp.int32(base[0])
        for q in range(1, 4):
            first = jnp.where(r == q, base[q], first)

        @pl.when(jnp.logical_and(live, j == 0))
        def _():
            def pack(zs):
                for z in zs:
                    at = jnp.minimum(first + z, sum(spans) - 1)
                    tile = kv_ref[:, at, :, pl.ds(HALF, 16), :].reshape(256, 128)
                    got = jnp.dot(pick_rows, tile, preferred_element_type=jnp.float32)
                    got = jnp.where(z <= kv // N, got, 0.0)
                    comp[pl.ds(z * 48, 48), :] = got.astype(jnp.bfloat16)

            pack((0, 1))
            pl.when(kv >= 2 * N)(lambda: pack((2, 3)))
            pl.when(kv >= 4 * N)(lambda: pack((4, 5, 6, 7)))

        @pl.when(jnp.logical_not(live))
        def _():
            out_ref[seq, rows] = jnp.zeros((BLK, PER * HEAD), jnp.bfloat16)

        @pl.when(live)
        def _():
            def fetch(p, count):
                b = ints_ref[seq, j, p]

                @pl.when(b >= 0)
                def _():
                    span = (b * 10923) >> 16
                    at = b - span * 6
                    t = jnp.where(at >= 3, 1, 0)
                    row = (at - t * 3) * BLK
                    buf[pl.ds(pl.multiple_of(count * BLK, BLK), BLK), :] = kv_ref[
                        t,
                        first + (span >> 3),
                        span & 7,
                        pl.ds(pl.multiple_of(row, BLK), BLK),
                        :,
                    ]

                return count + jnp.where(b >= 0, 1, 0)

            count = lax.fori_loop(0, PICKS, fetch, jnp.int32(0), unroll=True)
            parts = []
            for h in range(PER):
                two = main_ref[seq, rows, pl.ds((h // 2) * 128, 128)].astype(jnp.float32) * 0.125
                if h % 2:
                    two = pltpu.roll(two, 64, 1)
                parts.append(jnp.where(lane < HEAD, two, 0.0).astype(jnp.bfloat16))
            q = jnp.concatenate(parts, axis=0)

            def score(keys):
                return lax.dot_general(
                    q, keys, (((1,), (1,)), ((), ())), preferred_element_type=jnp.float32
                )

            spot = start + j * BLK + row_in
            own = main_ref[seq, rows, pl.ds(PER * HEAD, 128)]
            ks = lax.broadcasted_iota(jnp.int32, (1, BLK), 1)

            def run(most, far_too):
                keys = comp[pl.ds(0, most), :]
                cs = jnp.where(block_ends[:, :most] <= spot, score(keys), MASKED)
                ctop = jnp.max(cs, axis=-1, keepdims=True)
                cw = jnp.exp(cs - ctop)
                cn = jnp.maximum(jnp.sum(cw, axis=-1, keepdims=True), 1.0)
                cp = (cw * jnp.where(spot >= BLK - 1, 1.0 / cn, 0.0)).astype(jnp.bfloat16)
                co = jnp.dot(cp, keys, preferred_element_type=jnp.float32)

                os = jnp.where(ks <= row_in, score(own), MASKED)
                top = jnp.max(os, axis=-1, keepdims=True)
                if far_too:
                    far = buf[...]
                    spots = lax.broadcasted_iota(jnp.int32, (1, PICKS * BLK), 1)
                    fs = jnp.where(spots < count * BLK, score(far), MASKED)
                    top = jnp.maximum(top, jnp.max(fs, axis=-1, keepdims=True))
                ow = jnp.exp(os - top)
                total = jnp.sum(ow, axis=-1, keepdims=True)
                if far_too:
                    fw = jnp.exp(fs - top)
                    total = total + jnp.sum(fw, axis=-1, keepdims=True)
                inv = 1.0 / total
                so = jnp.dot((ow * inv).astype(jnp.bfloat16), own, preferred_element_type=jnp.float32)
                if far_too:
                    so = so + jnp.dot(
                        (fw * inv).astype(jnp.bfloat16), far, preferred_element_type=jnp.float32
                    )
                mixed = []
                g = gate_ref[seq, rows]
                for h in range(PER):
                    at = slice(h * BLK, (h + 1) * BLK)
                    mixed.append(g[:, h : h + 1] * co[at] + g[:, 4 + h : 5 + h] * so[at])
                for h in range(2):
                    pair = jnp.where(
                        lane < HEAD, pltpu.roll(mixed[2 * h], 64, 1), mixed[2 * h + 1]
                    )
                    out_ref[seq, rows, pl.ds(h * 128, 128)] = pair.astype(jnp.bfloat16)

            low, some = kv < 2 * N, count > 0
            for cond_low, most in ((low, 128), (jnp.logical_not(low), 384)):
                for cond_far, far_too in ((some, True), (jnp.logical_not(some), False)):
                    pl.when(jnp.logical_and(cond_low, cond_far))(
                        functools.partial(run, most, far_too)
                    )

        return carry

    buf[...] = jnp.zeros_like(buf)
    lax.fori_loop(0, 12, step, 0)


def attend(spans, order, gint, got, gates, gathered):
    vm = pl.BlockSpec(memory_space=VMEM)
    sm = pl.BlockSpec(memory_space=SMEM)
    c = jnp.arange(384, dtype=jnp.int32)
    z, t, y, j = c // 48, c % 48 // 24, c % 24 // 3, c % 3
    blocks = ((z * N + y) * 6 + t * 3 + j)[None]
    return pl.pallas_call(
        functools.partial(attend_kernel, spans),
        out_shape=jax.ShapeDtypeStruct((4, HALF, PER * HEAD), jnp.bfloat16),
        in_specs=[sm, sm, vm, vm, vm, vm],
        out_specs=vm,
        scratch_shapes=[
            pltpu.VMEM((PICKS * BLK, 2 * HEAD), jnp.bfloat16),
            pltpu.VMEM((384, 2 * HEAD), jnp.bfloat16),
        ],
        compiler_params=pltpu.CompilerParams(vmem_limit_bytes=(24 if sum(spans) < 20 else 48) << 20),
        name="attend",
    )(order, gint, got, gates, gathered, blocks)


def finish_kernel(len_ref, att_ref, wo_ref, out_ref, back, send_sems, recv_sems):
    dp, kv, tp = lax.axis_index("dp"), lax.axis_index("kv"), lax.axis_index("tp")
    barrier([{"dp": lax.rem(dp + d, 4)} for d in range(1, 4)])

    def copy(d):
        to = lax.rem(dp + d, 4)
        return pltpu.make_async_remote_copy(
            src_ref=att_ref.at[to],
            dst_ref=back.at[dp],
            send_sem=send_sems.at[d],
            recv_sem=recv_sems.at[d],
            device_id={"dp": to},
            device_id_type=MESH,
        )

    for d in (2, 1, 3):
        copy(d).start()
    back[dp] = att_ref[dp]

    def arrived(frm):
        d = lax.rem(dp + 4 - frm, 4)
        pltpu.make_async_remote_copy(
            src_ref=back.at[frm],
            dst_ref=back.at[frm],
            send_sem=send_sems.at[d],
            recv_sem=recv_sems.at[d],
            device_id={"dp": frm},
            device_id_type=MESH,
        ).wait_recv()

    spot = kv * (2 * HALF) + tp * HALF + lax.broadcasted_iota(jnp.int32, (HALF, 1), 0)
    alive = spot < len_ref[0]

    def tiles(t, last):
        cols = jnp.concatenate([back[2 * t], back[2 * t + 1]], axis=1)

        def tile(z, carry):
            w = wo_ref[t, z].reshape(256, 512)
            part = lax.dot_general(
                cols, w, (((1,), (1,)), ((), ())), preferred_element_type=jnp.float32
            ).astype(jnp.bfloat16)
            at = pl.ds(pl.multiple_of(z * 256, 256), 256)
            if last:
                both_sets = out_ref[:, at].astype(jnp.float32) + part.astype(jnp.float32)
                part = jnp.where(alive, both_sets, 0.0).astype(jnp.bfloat16)
            out_ref[:, at] = part
            return carry

        lax.fori_loop(0, N, tile, 0, unroll=2)

    near = dp // 2
    arrived(4 * near + 1 - dp)
    tiles(near, False)
    arrived(2 - 2 * near)
    arrived(3 - 2 * near)
    tiles(1 - near, True)
    for d in (1, 2, 3):
        copy(d).wait_send()


def finish(length, att, wo, number):
    vm = pl.BlockSpec(memory_space=VMEM)
    return pl.pallas_call(
        finish_kernel,
        out_shape=jax.ShapeDtypeStruct((HALF, 2048), jnp.bfloat16),
        in_specs=[pl.BlockSpec(memory_space=SMEM), vm, vm],
        out_specs=vm,
        scratch_shapes=[
            pltpu.VMEM((4, HALF, PER * HEAD), jnp.bfloat16),
            pltpu.SemaphoreType.DMA((4,)),
            pltpu.SemaphoreType.DMA((4,)),
        ],
        compiler_params=pltpu.CompilerParams(
            collective_id=number, has_side_effects=True, vmem_limit_bytes=24 << 20
        ),
        name="finish",
    )(length, att, wo)


def body(
    tokens, seq_lengths, block_picks, w_query, w_key, w_value, w_gate, w_ckey, w_cvalue, w_out
):
    x = tokens[0]
    dp = lax.axis_index("dp")
    low = lax.rem(dp, 2) == 0
    piece = jnp.where(
        low,
        jnp.concatenate([w_query[:, :256], w_key[:, :64], w_value[:, :64]], axis=1),
        jnp.concatenate([w_query[:, 256:], w_key[:, 64:], w_value[:, 64:]], axis=1),
    )
    picks = block_picks[0].transpose(1, 0, 2).reshape(2, 2, 3, PICKS)
    ints = jnp.pad(picks, ((0, 0), (0, 0), (0, 5), (0, 112)))
    row = lax.broadcasted_iota(jnp.int32, ints.shape, 2)
    ints = jnp.where(row == 7, seq_lengths[0], ints)
    toks, w_all, wo, gint = entry(x, piece, w_out.T, ints)
    toks = toks.reshape(4 * HALF, 2048)

    gate_cols = lax.dynamic_index_in_dim(w_gate.reshape(2048, 2, GROUPS, PER), dp, 2, keepdims=False)
    gates = jax.nn.sigmoid(
        jnp.dot(toks, gate_cols.reshape(2048, 8), preferred_element_type=jnp.float32)
    ).reshape(4, HALF, 8)
    qkv = jnp.dot(toks, w_all.reshape(2048, 384), preferred_element_type=jnp.float32)
    qkv = qkv.astype(jnp.bfloat16)
    flat = qkv.reshape(12, BLK, 384)
    ck = jnp.dot(
        flat[..., 256:320].reshape(12, BLK * HEAD), w_ckey, preferred_element_type=jnp.float32
    )
    cv = jnp.dot(
        flat[..., 320:].reshape(12, BLK * HEAD), w_cvalue, preferred_element_type=jnp.float32
    )
    pairs = jnp.concatenate([ck, cv], axis=1).astype(jnp.bfloat16).reshape(4, 3, 128)
    pairs = jnp.pad(pairs, ((0, 0), (0, 13), (0, 0)))
    got = qkv.reshape(4, HALF, 384)
    lens = gint[:, 7, 0]
    ids = jnp.arange(4, dtype=jnp.int32)
    ahead = (lens[None, :] > lens[:, None]) | (
        (lens[None, :] == lens[:, None]) & (ids[None, :] < ids[:, None])
    )
    rank = jnp.sum(ahead.astype(jnp.int32), axis=1)
    order = jnp.sum(jnp.where(rank[None, :] == ids[:, None], ids[None, :], 0), axis=1)
    ranked = jnp.sum(
        jnp.where(rank[None, :] == ids[:, None], lens[None, :], 0), axis=1
    )

    def run(spans, number, limit):
        gathered = gather_kv(order, got, pairs, spans, number, limit)
        att = attend(spans, order, gint, got, gates, gathered)
        return finish(seq_lengths, att, wo, number + 1)

    span = N * 384
    small = (ranked[1] <= 3 * span) & (ranked[2] <= 2 * span) & (ranked[3] <= span)
    out = lax.cond(
        small, lambda: run((8, 3, 2, 1), 2, 448), lambda: run((8, 8, 8, 8), 4, 600)
    )
    return out[None]


def solution(mesh):
    return jax.shard_map(
        body,
        mesh=mesh,
        in_specs=(
            P("dp", "kv", None),
            P("dp"),
            P("dp", "kv", "tp", None),
            P("kv", "tp"),
            P("kv", "tp"),
            P("kv", "tp"),
            P(),
            P(),
            P(),
            P("tp", "kv"),
        ),
        out_specs=P("dp", ("kv", "tp"), None),
        check_vma=False,
    )
```

```python
import functools

import jax
import jax.numpy as jnp
from jax import lax
from jax.experimental import pallas as pl
from jax.experimental.pallas import tpu as pltpu
from jax.sharding import PartitionSpec as P

MESH = pl.DeviceIdType.MESH

HEADS = 16
GROUPS = 4
PER = 4
HEAD = 64
BLK = 64
PICKS = 16
N = 8
ROWS = 208
HALF = 192
SPLIT = 112
MASKED = -1e30
VMEM = pltpu.MemorySpace.VMEM
SMEM = pltpu.MemorySpace.SMEM
HBM = pltpu.MemorySpace.HBM


def place():
    kv = lax.axis_index("kv")
    return kv // N, lax.rem(kv, N)


class Copies:
    def __init__(self, send_sems, recv_sems):
        self.send_sems, self.recv_sems, self.used, self.sent = send_sems, recv_sems, 0, []

    def slot(self):
        self.used += 1
        return self.used - 1

    def send(self, i, src, dst, device):
        copy = pltpu.make_async_remote_copy(
            src_ref=src,
            dst_ref=dst,
            send_sem=self.send_sems.at[i],
            recv_sem=self.recv_sems.at[i],
            device_id=device,
            device_id_type=MESH,
        )
        copy.start()

    def arrived(self, i, ref, device):
        pltpu.make_async_remote_copy(
            src_ref=ref,
            dst_ref=ref,
            send_sem=self.send_sems.at[i],
            recv_sem=self.recv_sems.at[i],
            device_id=device,
            device_id_type=MESH,
        ).wait_recv()

    def left(self, i, ref, device):
        pltpu.make_async_remote_copy(
            src_ref=ref,
            dst_ref=ref,
            send_sem=self.send_sems.at[i],
            recv_sem=self.recv_sems.at[i],
            device_id=device,
            device_id_type=MESH,
        ).wait_send()


def when(cond, fn):
    if cond is True:
        fn()
    elif cond is not False:
        pl.when(cond)(fn)


def both(a, b):
    if a is True:
        return b
    if b is True:
        return a
    if a is False or b is False:
        return False
    return jnp.logical_and(a, b)


def wrap(i):
    return lax.rem(i + N, N)


def barrier(kinds):
    sem = pltpu.get_barrier_semaphore()
    for device in kinds:
        pl.semaphore_signal(sem, inc=1, device_id=device, device_id_type=MESH)
    pl.semaphore_wait(sem, len(kinds))


def plane_partners(z, y):
    return [{"kv": z * N + wrap(y + d)} for d in range(1, N)] + [
        {"kv": wrap(z + d) * N + y} for d in range(1, N)
    ]


class Gather:
    def __init__(
        self, copies, src, view, rows, causal, pair, parts=(True, True), tie=False, only=True
    ):
        self.c, self.src, self.view, self.rows, self.causal = copies, src, view, rows, causal
        self.pair, self.parts, self.tie = pair, parts, tie
        self.z, self.y = place()
        self.live = True if rows == N else self.z < rows
        self.only = only
        self.waits = []
        self.pair_waits = []
        self.flight = {}
        if not causal:
            self.subs_b = [(0, 4), (4, 4)]
        elif rows == N:
            self.subs_b = [(0, 1), (1, 1), (2, 2), (4, 2), (6, 2)]
        else:
            self.subs_b = [(i, 1) for i in range(rows)]

    def dev(self, z, y):
        return {"kv": z * N + y}

    def transfer(self, cond_send, src, dst, device, cond_recv, got):
        i = self.c.slot()
        cond_send, cond_recv = both(cond_send, self.only), both(cond_recv, self.only)
        when(cond_send, lambda: self.c.send(i, src, dst, device))
        self.waits.append((i, cond_send, src, device))
        return (i, cond_recv, got, device)

    def take(self, t):
        i, cond, ref, device = t
        when(cond, lambda: self.c.arrived(i, ref, device))

    def mirror(self, cond, ref):
        if self.pair is None:
            return
        i = self.c.slot()
        send, recv = cond, cond
        if self.only is not True:
            send, recv = self.only, jnp.logical_not(self.only)
        when(send, lambda: self.c.send(i, ref, ref, self.pair))
        self.pair_waits.append((i, send, recv, ref))

    def first(self):
        z, y = self.z, self.y
        self.a1, self.b1 = [], []
        for d in range(1, N) if self.parts[0] else ():
            self.a1.append(
                self.transfer(
                    self.live,
                    self.src(0),
                    self.view(z, 1, y, 1, 0),
                    self.dev(z, wrap(y + d)),
                    self.live,
                    self.view(z, 1, wrap(y - d), 1, 0),
                )
            )
        reach = N if not self.causal else self.rows
        for d in range(1, reach) if self.parts[1] else ():
            cs = True if not self.causal else z + d < self.rows
            cr = True if not self.causal else both(self.live, z - d >= 0)
            self.b1.append(
                self.transfer(
                    cs,
                    self.src(1),
                    self.view(z, 1, y, 1, 1),
                    self.dev(wrap(z + d), y),
                    cr,
                    self.view(wrap(z - d), 1, y, 1, 1),
                )
            )

    def ring_y(self, k, z0, nz, part, right, cond):
        z, y = self.z, self.y
        if right:
            o, got, to = wrap(y - (k - 1)), wrap(y - k), wrap(y + 1)
        else:
            o, got, to = lax.rem(y + k - 1, N), lax.rem(y + k, N), wrap(y - 1)
        return self.transfer(
            cond,
            self.view(z0, nz, o, 1, part),
            self.view(z0, nz, o, 1, part),
            self.dev(z, to),
            cond,
            self.view(z0, nz, got, 1, part),
        )

    def hop_a(self, right, sub, k, depth):
        z, y = self.z, self.y
        y0, ny = (sub * 4, 4)
        if right:
            o, got, to = wrap(z - (k - 1)), wrap(z - k), wrap(z + 1)
            cs = both(z - (k - 1) >= 0, z + 1 < self.rows) if self.causal else True
            cr = both(self.live, z - k >= 0) if self.causal else True
        else:
            o, got, to = wrap(z + k - 1), lax.rem(z + k, N), wrap(z - 1)
            cs = o < depth if self.causal else True
            cr = got < depth if self.causal else True
        return self.transfer(
            cs,
            self.view(o, 1, y0, ny, 0),
            self.view(o, 1, y0, ny, 0),
            self.dev(to, y),
            cr,
            self.view(got, 1, y0, ny, 0),
        )

    def hop_b(self, right, sub, k):
        z0, nz = self.subs_b[sub]
        cond = self.live
        if self.causal and z0 > 0:
            cond = both(cond, self.z >= z0)
        return self.ring_y(k, z0, nz, 1, right, cond)

    def depth_a(self, right, sub):
        if self.rows < N:
            return self.rows - 1 if right else 0
        return 4 if right == (sub == 0) else 3

    def depth_b(self, right, sub):
        return 4 if right == ((sub % 2 == 0) != self.tie) else 3

    def hop(self, k):
        steps = []
        order = [("a", 0), ("b", 0), ("b", 1), ("a", 1)] + [("b", i) for i in range(2, 5)]
        begun = set()
        for ring, s in order:
            if s >= (2 if ring == "a" else len(self.subs_b)) or not self.parts[ring == "b"]:
                continue
            if k == 1 and ring not in begun:
                begun.add(ring)
                steps.append(lambda ring=ring: self.begin(ring))
            for r in (True, False):
                steps.append(lambda ring=ring, s=s, r=r: self.lane(ring, s, r, k))
        return steps

    def begin(self, ring):
        for t in self.a1 if ring == "a" else self.b1:
            self.take(t)

    def lane(self, ring, s, r, k):
        depth = self.depth_a(r, s) if ring == "a" else self.depth_b(r, s)
        got = None
        if 1 < k <= depth + 1:
            got = self.flight[ring, r, s]
            self.take(got)
        if k <= depth:
            self.flight[ring, r, s] = (
                self.hop_a(r, s, k, depth) if ring == "a" else self.hop_b(r, s, k)
            )
        if got is not None:
            self.mirror(got[1], got[2])
        if k == 1 and r:
            if ring == "a":
                self.mirror(self.live, self.view(self.z, 1, s * 4, 4, 0))
            else:
                z0, nz = self.subs_b[s]
                cond = both(self.live, self.z >= z0) if z0 and self.causal else self.live
                self.mirror(cond, self.view(z0, nz, self.y, 1, 1))

    def last(self):
        for i, send, recv, ref in self.pair_waits:
            when(recv, lambda: self.c.arrived(i, ref, self.pair))
            when(send, lambda: self.c.left(i, ref, self.pair))
        for i, cond, ref, device in self.waits:
            when(cond, lambda: self.c.left(i, ref, device))


def spread_partners(dp, tp):
    return [{"dp": lax.rem(dp + e // 2, 4), "tp": lax.rem(tp + e % 2, 2)} for e in range(1, 8)]


def entry_kernel(
    x_ref,
    w_ref,
    o_ref,
    ints_ref,
    wg_ref,
    qkv_ref,
    gate_ref,
    wo_ref,
    gint_ref,
    tok_ref,
    wall_ref,
    wcat_ref,
    wg_buf,
    send_sems,
    recv_sems,
    int_sems,
    local_sem,
    gate_sem,
):
    z, y = place()
    dp, tp = lax.axis_index("dp"), lax.axis_index("tp")
    pair = {"tp": 1 - tp}
    owner = dp // 2 == tp
    mine = x_ref.at[pl.ds(pl.multiple_of(tp * HALF, HALF), HALF)]
    local = pltpu.make_async_copy(mine, tok_ref.at[dp], local_sem)
    local.start()
    gate_copy = pltpu.make_async_copy(wg_ref, wg_buf, gate_sem)
    gate_copy.start()
    wo_ref[tp, z, y] = o_ref[...]

    @pl.when(owner)
    def _():
        wall_ref[z, y] = w_ref[...]

    barrier(plane_partners(z, y) + spread_partners(dp, tp))
    c = Copies(send_sems, recv_sems)

    left, right = lax.rem(dp + 3, 4), lax.rem(dp + 1, 4)
    part = HALF // 2
    first = {}
    for way, to, subs in (("r", right, (0, 1)), ("l", left, (1, 0))):
        for sub in subs:
            i = c.slot()
            src = x_ref.at[pl.ds(pl.multiple_of(tp * HALF + sub * part, part), part)]
            c.send(i, src, tok_ref.at[dp, pl.ds(sub * part, part)], {"dp": to})
            first[way, sub] = (i, src, to)

    def int_copy(gl, h):
        return pltpu.make_async_remote_copy(
            src_ref=ints_ref.at[gl, h],
            dst_ref=gint_ref.at[dp],
            send_sem=int_sems.at[gl * 2 + h],
            recv_sem=int_sems.at[4 + dp],
            device_id={"dp": 2 * tp + gl, "tp": jnp.int32(h)},
            device_id_type=MESH,
        )

    def is_own(gl, h):
        return jnp.logical_and(2 * tp + gl == dp, tp == h)

    for gl in range(2):
        for h in range(2):

            def go(gl=gl, h=h):
                int_copy(gl, h).start()

            def keep(gl=gl, h=h):
                gint_ref[dp] = ints_ref[gl, h]

            pl.when(jnp.logical_not(is_own(gl, h)))(go)
            pl.when(is_own(gl, h))(keep)

    jobs = []
    for src_ref, out_ref, only in ((o_ref, wo_ref.at[tp], True), (w_ref, wall_ref, owner)):
        half = src_ref.shape[0] // 2

        def src(part, src_ref=src_ref, half=half):
            return src_ref.at[pl.ds(part * half, half)]

        def view(z0, nz, y0, ny, part, out_ref=out_ref, half=half):
            zi = z0 if nz == 1 else pl.ds(z0, nz)
            yi = y0 if ny == 1 else pl.ds(y0, ny)
            return out_ref.at[zi, yi, pl.ds(part * half, half)]

        jobs.append(Gather(c, src, view, N, False, pair, only=only))
    for g in jobs:
        g.first()
    second = []

    def onward(way, sub, frm, to):
        i = first[way, sub][0]
        ref = tok_ref.at[frm, pl.ds(sub * part, part)]
        c.arrived(i, ref, {"dp": to})
        i2 = c.slot()
        c.send(i2, ref, ref, {"dp": to})
        second.append((i2, ref, sub, to))

    for k in range(1, 6):
        for g in jobs:
            for step in g.hop(k):
                step()
        if k == 2:
            onward("r", 0, left, right)
            onward("l", 1, right, left)
    assert c.used <= send_sems.shape[0], c.used
    for g in jobs:
        g.last()

    frm_col = lax.broadcasted_iota(jnp.int32, (2 * HEADS, 128), 0)
    to_col = lax.broadcasted_iota(jnp.int32, (2 * HEADS, 128), 1)
    wanted = (to_col >> 2) * HEADS + dp * PER + (to_col & 3)
    chosen = jnp.logical_and(frm_col == wanted, to_col < 8)
    gate_copy.wait()
    width = wall_ref.shape[3]
    wcat_ref[:, pl.ds(0, width)] = wall_ref[...].reshape(wcat_ref.shape[0], width)
    wcat_ref[:, pl.ds(width, 128)] = lax.dot_general(
        wg_buf[...],
        jnp.where(chosen, 1.0, 0.0).astype(jnp.bfloat16),
        (((0,), (0,)), ((), ())),
        preferred_element_type=jnp.float32,
    ).astype(jnp.bfloat16)

    def project(q):
        got = jnp.dot(tok_ref[q], wcat_ref[...], preferred_element_type=jnp.float32)
        qkv_ref[q] = got[:, :width].astype(jnp.bfloat16)
        gate_ref[q] = lax.logistic(got[:, width : width + 16])

    local.wait()
    project(dp)
    for q in range(4):

        def take(q=q):
            ref = gint_ref.at[q]
            pltpu.make_async_remote_copy(
                src_ref=ref,
                dst_ref=ref,
                send_sem=int_sems.at[0],
                recv_sem=int_sems.at[4 + q],
                device_id={"dp": jnp.int32(q), "tp": tp},
                device_id_type=MESH,
            ).wait_recv()

        pl.when(jnp.logical_not(jnp.logical_and(q == dp, owner)))(take)
    for gl in range(2):
        for h in range(2):
            pl.when(jnp.logical_not(is_own(gl, h)))(lambda gl=gl, h=h: int_copy(gl, h).wait_send())
    for way, sub, frm, to in (("r", 1, left, right), ("l", 0, right, left)):
        c.arrived(first[way, sub][0], tok_ref.at[frm, pl.ds(sub * part, part)], {"dp": to})
        project(frm)
    far = lax.rem(dp + 2, 4)
    for i2, ref, sub, to in second:
        c.arrived(i2, tok_ref.at[far, pl.ds(sub * part, part)], {"dp": to})
    project(far)
    for i, src, to in first.values():
        c.left(i, src, {"dp": to})
    for i2, ref, sub, to in second:
        c.left(i2, ref, {"dp": to})


def entry(x, w, o, ints, wg):
    vm = pl.BlockSpec(memory_space=VMEM)
    hbm = pl.BlockSpec(memory_space=HBM)
    return pl.pallas_call(
        entry_kernel,
        out_shape=[
            jax.ShapeDtypeStruct((4, HALF, w.shape[1]), x.dtype),
            jax.ShapeDtypeStruct((4, HALF, 16), jnp.float32),
            jax.ShapeDtypeStruct((2, N, N) + o.shape, o.dtype),
            jax.ShapeDtypeStruct((4,) + ints.shape[2:], ints.dtype),
        ],
        in_specs=[hbm, vm, vm, vm, hbm],
        out_specs=[vm] * 4,
        scratch_shapes=[
            pltpu.VMEM((4, HALF, x.shape[1]), x.dtype),
            pltpu.VMEM((N, N) + w.shape, w.dtype),
            pltpu.VMEM((x.shape[1], w.shape[1] + 128), w.dtype),
            pltpu.VMEM(wg.shape, wg.dtype),
            pltpu.SemaphoreType.DMA((192,)),
            pltpu.SemaphoreType.DMA((192,)),
            pltpu.SemaphoreType.DMA((8,)),
            pltpu.SemaphoreType.DMA,
            pltpu.SemaphoreType.DMA,
        ],
        compiler_params=pltpu.CompilerParams(
            collective_id=0, has_side_effects=True, vmem_limit_bytes=60 << 20
        ),
        cost_estimate=pl.CostEstimate(
            flops=30_000_000_000, bytes_accessed=8 << 20, transcendentals=0
        ),
        name="entry",
    )(x, w, o, ints, wg)


def bases(spans):
    return [sum(spans[:r]) for r in range(4)]


def kv_kernel(spans, order_ref, got_ref, pairs_ref, out_ref, own, send_sems, recv_sems):
    z, y = place()
    tp = lax.axis_index("tp")
    pair = {"tp": 1 - tp}
    base = bases(spans)
    for r, rows in enumerate(spans):

        def fill(r=r):
            seq = order_ref[r]
            piece = got_ref[seq, :, pl.ds(PER * HEAD, 2 * HEAD)]
            pairs = pairs_ref[seq]
            for ref in (own.at[r], out_ref.at[tp, base[r] + z, y]):
                ref[pl.ds(0, HALF)] = piece
                ref[pl.ds(HALF, ROWS - HALF)] = pairs

        when(True if rows == N else z < rows, fill)
    barrier(plane_partners(z, y) + [pair])
    c = Copies(send_sems, recv_sems)
    jobs = []
    for r, rows in enumerate(spans):

        split = SPLIT if r == 0 else 0

        def part_rows(part, split=split):
            return pl.ds(0, split) if part == 0 else pl.ds(split, ROWS - split)

        def src(part, r=r, part_rows=part_rows):
            return own.at[r, part_rows(part)]

        def view(z0, nz, y0, ny, part, r=r, part_rows=part_rows):
            zi = base[r] + z0 if nz == 1 else pl.ds(base[r] + z0, nz)
            yi = y0 if ny == 1 else pl.ds(y0, ny)
            return out_ref.at[tp, zi, yi, part_rows(part)]

        jobs.append(Gather(c, src, view, rows, True, pair, (r == 0, True), r % 2 == 1))
    for g in jobs:
        g.first()
    for k in range(1, 6):
        for g in jobs:
            for step in g.hop(k):
                step()
    assert c.used <= send_sems.shape[0], c.used
    for g in jobs:
        g.last()


def gather_kv(order, got, pairs, spans, number, limit):
    vm = pl.BlockSpec(memory_space=VMEM)
    return pl.pallas_call(
        functools.partial(kv_kernel, spans),
        out_shape=jax.ShapeDtypeStruct((2, sum(spans), N, ROWS, 2 * HEAD), got.dtype),
        in_specs=[pl.BlockSpec(memory_space=SMEM), vm, vm],
        out_specs=vm,
        scratch_shapes=[
            pltpu.VMEM((4, ROWS, 2 * HEAD), jnp.bfloat16),
            pltpu.SemaphoreType.DMA((limit,)),
            pltpu.SemaphoreType.DMA((limit,)),
        ],
        compiler_params=pltpu.CompilerParams(
            collective_id=number,
            has_side_effects=True,
            vmem_limit_bytes=(24 if sum(spans) < 20 else 40) << 20,
        ),
        cost_estimate=pl.CostEstimate(
            flops=30_000_000_000, bytes_accessed=8 << 20, transcendentals=0
        ),
        name="gather_kv",
    )(order, got, pairs)


def attend_kernel(
    spans, order_ref, ints_ref, main_ref, gate_ref, kv_ref, block_ref, out_ref, buf, comp
):
    kv, tp = lax.axis_index("kv"), lax.axis_index("tp")
    start = kv * (2 * HALF) + tp * HALF
    base = bases(spans)
    lane = lax.broadcasted_iota(jnp.int32, (BLK, 128), 1)
    row_in = lax.rem(lax.broadcasted_iota(jnp.int32, (PER * BLK, 1), 0), BLK)
    comp[...] = jnp.zeros_like(comp)
    to_row = lax.broadcasted_iota(jnp.int32, (48, 256), 0)
    from_row = lax.broadcasted_iota(jnp.int32, (48, 256), 1)
    piece = (to_row * 21846) >> 16
    pick_rows = jnp.where(from_row == piece * 16 + (to_row - piece * 3), 1.0, 0.0).astype(jnp.bfloat16)
    block_ends = block_ref[...] * BLK + (BLK - 1)

    def step(n, carry):
        r = (n * 21846) >> 16
        j = n - r * 3
        seq = order_ref[r]
        rows = pl.ds(pl.multiple_of(j * BLK, BLK), BLK)
        live = start < ints_ref[seq, 7, 0]
        first = jnp.int32(base[0])
        for q in range(1, 4):
            first = jnp.where(r == q, base[q], first)

        @pl.when(jnp.logical_and(live, j == 0))
        def _():
            def pack(zs):
                for z in zs:
                    at = jnp.minimum(first + z, sum(spans) - 1)
                    tile = kv_ref[:, at, :, pl.ds(HALF, 16), :].reshape(256, 128)
                    got = jnp.dot(pick_rows, tile, preferred_element_type=jnp.float32)
                    got = jnp.where(z <= kv // N, got, 0.0)
                    comp[pl.ds(z * 48, 48), :] = got.astype(jnp.bfloat16)

            pack((0, 1))
            pl.when(kv >= 2 * N)(lambda: pack((2, 3)))
            pl.when(kv >= 4 * N)(lambda: pack((4, 5, 6, 7)))

        @pl.when(jnp.logical_not(live))
        def _():
            out_ref[seq, rows] = jnp.zeros((BLK, PER * HEAD), jnp.bfloat16)

        @pl.when(live)
        def _():
            def fetch(p, count):
                b = ints_ref[seq, j, p]

                @pl.when(b >= 0)
                def _():
                    span = (b * 10923) >> 16
                    at = b - span * 6
                    t = jnp.where(at >= 3, 1, 0)
                    row = (at - t * 3) * BLK
                    buf[pl.ds(pl.multiple_of(count * BLK, BLK), BLK), :] = kv_ref[
                        t,
                        first + (span >> 3),
                        span & 7,
                        pl.ds(pl.multiple_of(row, BLK), BLK),
                        :,
                    ]

                return count + jnp.where(b >= 0, 1, 0)

            count = ints_ref[seq, j, PICKS]

            @pl.when(count > 0)
            def _():
                lax.fori_loop(0, PICKS, fetch, jnp.int32(0), unroll=True)

            parts = []
            for h in range(PER):
                two = main_ref[seq, rows, pl.ds((h // 2) * 128, 128)].astype(jnp.float32) * 0.125
                if h % 2:
                    two = pltpu.roll(two, 64, 1)
                parts.append(jnp.where(lane < HEAD, two, 0.0).astype(jnp.bfloat16))
            q = jnp.concatenate(parts, axis=0)

            def score(keys):
                return lax.dot_general(
                    q, keys, (((1,), (1,)), ((), ())), preferred_element_type=jnp.float32
                )

            spot = start + j * BLK + row_in
            own = main_ref[seq, rows, pl.ds(PER * HEAD, 128)]
            ks = lax.broadcasted_iota(jnp.int32, (1, BLK), 1)

            def run(most, far_too):
                keys = comp[pl.ds(0, most), :]
                cs = jnp.where(block_ends[:, :most] <= spot, score(keys), MASKED)
                ctop = jnp.max(cs, axis=-1, keepdims=True)
                cw = jnp.exp(cs - ctop)
                cn = jnp.maximum(jnp.sum(cw, axis=-1, keepdims=True), 1.0)
                cp = (cw * jnp.where(spot >= BLK - 1, 1.0 / cn, 0.0)).astype(jnp.bfloat16)
                co = jnp.dot(cp, keys, preferred_element_type=jnp.float32)

                os = jnp.where(ks <= row_in, score(own), MASKED)
                top = jnp.max(os, axis=-1, keepdims=True)
                if far_too:
                    far = buf[...]
                    spots = lax.broadcasted_iota(jnp.int32, (1, PICKS * BLK), 1)
                    fs = jnp.where(spots < count * BLK, score(far), MASKED)
                    top = jnp.maximum(top, jnp.max(fs, axis=-1, keepdims=True))
                ow = jnp.exp(os - top)
                total = jnp.sum(ow, axis=-1, keepdims=True)
                if far_too:
                    fw = jnp.exp(fs - top)
                    total = total + jnp.sum(fw, axis=-1, keepdims=True)
                inv = 1.0 / total
                so = jnp.dot((ow * inv).astype(jnp.bfloat16), own, preferred_element_type=jnp.float32)
                if far_too:
                    so = so + jnp.dot(
                        (fw * inv).astype(jnp.bfloat16), far, preferred_element_type=jnp.float32
                    )
                mixed = []
                g = gate_ref[seq, rows]
                for h in range(PER):
                    at = slice(h * BLK, (h + 1) * BLK)
                    mixed.append(g[:, h : h + 1] * co[at] + g[:, 4 + h : 5 + h] * so[at])
                for h in range(2):
                    pair = jnp.where(
                        lane < HEAD, pltpu.roll(mixed[2 * h], 64, 1), mixed[2 * h + 1]
                    )
                    out_ref[seq, rows, pl.ds(h * 128, 128)] = pair.astype(jnp.bfloat16)

            low, some = kv < 2 * N, count > 0
            for cond_low, most in ((low, 128), (jnp.logical_not(low), 384)):
                for cond_far, far_too in ((some, True), (jnp.logical_not(some), False)):
                    pl.when(jnp.logical_and(cond_low, cond_far))(
                        functools.partial(run, most, far_too)
                    )

        return carry

    buf[...] = jnp.zeros_like(buf)
    lax.fori_loop(0, 12, step, 0)


def attend(spans, order, gint, got, gates, gathered):
    vm = pl.BlockSpec(memory_space=VMEM)
    sm = pl.BlockSpec(memory_space=SMEM)
    c = jnp.arange(384, dtype=jnp.int32)
    z, t, y, j = c // 48, c % 48 // 24, c % 24 // 3, c % 3
    blocks = ((z * N + y) * 6 + t * 3 + j)[None]
    return pl.pallas_call(
        functools.partial(attend_kernel, spans),
        out_shape=jax.ShapeDtypeStruct((4, HALF, PER * HEAD), jnp.bfloat16),
        in_specs=[sm, sm, vm, vm, vm, vm],
        out_specs=vm,
        scratch_shapes=[
            pltpu.VMEM((PICKS * BLK, 2 * HEAD), jnp.bfloat16),
            pltpu.VMEM((384, 2 * HEAD), jnp.bfloat16),
        ],
        compiler_params=pltpu.CompilerParams(vmem_limit_bytes=(24 if sum(spans) < 20 else 48) << 20),
        name="attend",
    )(order, gint, got, gates, gathered, blocks)


def finish_kernel(len_ref, att_ref, wo_ref, out_ref, back, send_sems, recv_sems):
    dp, kv, tp = lax.axis_index("dp"), lax.axis_index("kv"), lax.axis_index("tp")
    barrier([{"dp": lax.rem(dp + d, 4)} for d in range(1, 4)])

    def copy(d):
        to = lax.rem(dp + d, 4)
        return pltpu.make_async_remote_copy(
            src_ref=att_ref.at[to],
            dst_ref=back.at[dp],
            send_sem=send_sems.at[d],
            recv_sem=recv_sems.at[d],
            device_id={"dp": to},
            device_id_type=MESH,
        )

    for d in (2, 1, 3):
        copy(d).start()
    back[dp] = att_ref[dp]

    def arrived(frm):
        d = lax.rem(dp + 4 - frm, 4)
        pltpu.make_async_remote_copy(
            src_ref=back.at[frm],
            dst_ref=back.at[frm],
            send_sem=send_sems.at[d],
            recv_sem=recv_sems.at[d],
            device_id={"dp": frm},
            device_id_type=MESH,
        ).wait_recv()

    spot = kv * (2 * HALF) + tp * HALF + lax.broadcasted_iota(jnp.int32, (HALF, 1), 0)
    alive = spot < len_ref[0]

    def tiles(t, last):
        cols = jnp.concatenate([back[2 * t], back[2 * t + 1]], axis=1)

        def tile(z, carry):
            w = wo_ref[t, z].reshape(256, 512)
            part = lax.dot_general(
                cols, w, (((1,), (1,)), ((), ())), preferred_element_type=jnp.float32
            ).astype(jnp.bfloat16)
            at = pl.ds(pl.multiple_of(z * 256, 256), 256)
            if last:
                both_sets = out_ref[:, at].astype(jnp.float32) + part.astype(jnp.float32)
                part = jnp.where(alive, both_sets, 0.0).astype(jnp.bfloat16)
            out_ref[:, at] = part
            return carry

        lax.fori_loop(0, N, tile, 0, unroll=2)

    near = dp // 2
    arrived(4 * near + 1 - dp)
    tiles(near, False)
    arrived(2 - 2 * near)
    arrived(3 - 2 * near)
    tiles(1 - near, True)
    for d in (1, 2, 3):
        copy(d).wait_send()


def finish(length, att, wo, number):
    vm = pl.BlockSpec(memory_space=VMEM)
    return pl.pallas_call(
        finish_kernel,
        out_shape=jax.ShapeDtypeStruct((HALF, 2048), jnp.bfloat16),
        in_specs=[pl.BlockSpec(memory_space=SMEM), vm, vm],
        out_specs=vm,
        scratch_shapes=[
            pltpu.VMEM((4, HALF, PER * HEAD), jnp.bfloat16),
            pltpu.SemaphoreType.DMA((4,)),
            pltpu.SemaphoreType.DMA((4,)),
        ],
        compiler_params=pltpu.CompilerParams(
            collective_id=number, has_side_effects=True, vmem_limit_bytes=24 << 20
        ),
        name="finish",
    )(length, att, wo)


def body(
    tokens, seq_lengths, block_picks, w_query, w_key, w_value, w_gate, w_ckey, w_cvalue, w_out
):
    x = tokens[0]
    dp = lax.axis_index("dp")
    low = lax.rem(dp, 2) == 0
    piece = jnp.where(
        low,
        jnp.concatenate([w_query[:, :256], w_key[:, :64], w_value[:, :64]], axis=1),
        jnp.concatenate([w_query[:, 256:], w_key[:, 64:], w_value[:, 64:]], axis=1),
    )
    picks = block_picks[0].transpose(1, 0, 2).reshape(2, 2, 3, PICKS)
    valid = jnp.sum((picks >= 0).astype(jnp.int32), axis=3, keepdims=True)
    ints = jnp.pad(picks, ((0, 0), (0, 0), (0, 5), (0, 112)))
    valid = jnp.pad(valid, ((0, 0), (0, 0), (0, 5), (0, 0)))
    row = lax.broadcasted_iota(jnp.int32, ints.shape, 2)
    col = lax.broadcasted_iota(jnp.int32, ints.shape, 3)
    ints = jnp.where(row == 7, seq_lengths[0], jnp.where(col == PICKS, valid, ints))
    got, gates, wo, gint = entry(x, piece, w_out.T, ints, w_gate.T)

    qkv = got.reshape(4 * HALF, 384)
    flat = qkv.reshape(12, BLK, 384)
    ck = jnp.dot(
        flat[..., 256:320].reshape(12, BLK * HEAD), w_ckey, preferred_element_type=jnp.float32
    )
    cv = jnp.dot(
        flat[..., 320:].reshape(12, BLK * HEAD), w_cvalue, preferred_element_type=jnp.float32
    )
    pairs = jnp.concatenate([ck, cv], axis=1).astype(jnp.bfloat16).reshape(4, 3, 128)
    pairs = jnp.pad(pairs, ((0, 0), (0, 13), (0, 0)))
    lens = gint[:, 7, 0]
    ids = jnp.arange(4, dtype=jnp.int32)
    ahead = (lens[None, :] > lens[:, None]) | (
        (lens[None, :] == lens[:, None]) & (ids[None, :] < ids[:, None])
    )
    rank = jnp.sum(ahead.astype(jnp.int32), axis=1)
    order = jnp.sum(jnp.where(rank[None, :] == ids[:, None], ids[None, :], 0), axis=1)
    ranked = jnp.sum(
        jnp.where(rank[None, :] == ids[:, None], lens[None, :], 0), axis=1
    )

    def run(spans, number, limit):
        gathered = gather_kv(order, got, pairs, spans, number, limit)
        att = attend(spans, order, gint, got, gates, gathered)
        return finish(seq_lengths, att, wo, number + 1)

    span = N * 384
    small = (ranked[1] <= 3 * span) & (ranked[2] <= 2 * span) & (ranked[3] <= span)
    out = lax.cond(
        small, lambda: run((8, 3, 2, 1), 2, 448), lambda: run((8, 8, 8, 8), 4, 600)
    )
    return out[None]


def solution(mesh):
    return jax.shard_map(
        body,
        mesh=mesh,
        in_specs=(
            P("dp", "kv", None),
            P("dp"),
            P("dp", "kv", "tp", None),
            P("kv", "tp"),
            P("kv", "tp"),
            P("kv", "tp"),
            P(),
            P(),
            P(),
            P("tp", "kv"),
        ),
        out_specs=P("dp", ("kv", "tp"), None),
        check_vma=False,
    )
```

```python
import functools

import jax
import jax.numpy as jnp
from jax import lax
from jax.experimental import pallas as pl
from jax.experimental.pallas import tpu as pltpu
from jax.sharding import PartitionSpec as P

MESH = pl.DeviceIdType.MESH

HEADS = 16
GROUPS = 4
PER = 4
HEAD = 64
BLK = 64
PICKS = 16
N = 8
ROWS = 208
HALF = 192
SPLIT = 96
MASKED = -1e30
VMEM = pltpu.MemorySpace.VMEM
SMEM = pltpu.MemorySpace.SMEM
HBM = pltpu.MemorySpace.HBM


def place():
    kv = lax.axis_index("kv")
    return kv // N, lax.rem(kv, N)


class Copies:
    def __init__(self, send_sems, recv_sems):
        self.send_sems, self.recv_sems, self.used, self.sent = send_sems, recv_sems, 0, []

    def slot(self):
        self.used += 1
        return self.used - 1

    def send(self, i, src, dst, device):
        copy = pltpu.make_async_remote_copy(
            src_ref=src,
            dst_ref=dst,
            send_sem=self.send_sems.at[i],
            recv_sem=self.recv_sems.at[i],
            device_id=device,
            device_id_type=MESH,
        )
        copy.start()

    def arrived(self, i, ref, device):
        pltpu.make_async_remote_copy(
            src_ref=ref,
            dst_ref=ref,
            send_sem=self.send_sems.at[i],
            recv_sem=self.recv_sems.at[i],
            device_id=device,
            device_id_type=MESH,
        ).wait_recv()

    def left(self, i, ref, device):
        pltpu.make_async_remote_copy(
            src_ref=ref,
            dst_ref=ref,
            send_sem=self.send_sems.at[i],
            recv_sem=self.recv_sems.at[i],
            device_id=device,
            device_id_type=MESH,
        ).wait_send()


def when(cond, fn):
    if cond is True:
        fn()
    elif cond is not False:
        pl.when(cond)(fn)


def both(a, b):
    if a is True:
        return b
    if b is True:
        return a
    if a is False or b is False:
        return False
    return jnp.logical_and(a, b)


def wrap(i):
    return lax.rem(i + N, N)


def barrier(kinds):
    sem = pltpu.get_barrier_semaphore()
    for device in kinds:
        pl.semaphore_signal(sem, inc=1, device_id=device, device_id_type=MESH)
    pl.semaphore_wait(sem, len(kinds))


def plane_partners(z, y):
    return [{"kv": z * N + wrap(y + d)} for d in range(1, N)] + [
        {"kv": wrap(z + d) * N + y} for d in range(1, N)
    ]


class Gather:
    def __init__(
        self, copies, src, view, rows, causal, pair, parts=(True, True), tie=False, only=True
    ):
        self.c, self.src, self.view, self.rows, self.causal = copies, src, view, rows, causal
        self.pair, self.parts, self.tie = pair, parts, tie
        self.z, self.y = place()
        self.live = True if rows == N else self.z < rows
        self.only = only
        self.waits = []
        self.pair_waits = []
        self.flight = {}
        if not causal:
            self.subs_b = [(0, 4), (4, 4)]
        elif rows == N:
            self.subs_b = [(0, 1), (1, 1), (2, 2), (4, 2), (6, 2)]
        else:
            self.subs_b = [(i, 1) for i in range(rows)]

    def dev(self, z, y):
        return {"kv": z * N + y}

    def transfer(self, cond_send, src, dst, device, cond_recv, got):
        i = self.c.slot()
        cond_send, cond_recv = both(cond_send, self.only), both(cond_recv, self.only)
        when(cond_send, lambda: self.c.send(i, src, dst, device))
        self.waits.append((i, cond_send, src, device))
        return (i, cond_recv, got, device)

    def take(self, t):
        i, cond, ref, device = t
        when(cond, lambda: self.c.arrived(i, ref, device))

    def mirror(self, cond, ref):
        if self.pair is None:
            return
        i = self.c.slot()
        send, recv = cond, cond
        if self.only is not True:
            send, recv = self.only, jnp.logical_not(self.only)
        when(send, lambda: self.c.send(i, ref, ref, self.pair))
        self.pair_waits.append((i, send, recv, ref))

    def first(self):
        z, y = self.z, self.y
        self.a1, self.b1 = [], []
        for d in range(1, N) if self.parts[0] else ():
            self.a1.append(
                self.transfer(
                    self.live,
                    self.src(0),
                    self.view(z, 1, y, 1, 0),
                    self.dev(z, wrap(y + d)),
                    self.live,
                    self.view(z, 1, wrap(y - d), 1, 0),
                )
            )
        reach = N if not self.causal else self.rows
        for d in range(1, reach) if self.parts[1] else ():
            cs = True if not self.causal else z + d < self.rows
            cr = True if not self.causal else both(self.live, z - d >= 0)
            self.b1.append(
                self.transfer(
                    cs,
                    self.src(1),
                    self.view(z, 1, y, 1, 1),
                    self.dev(wrap(z + d), y),
                    cr,
                    self.view(wrap(z - d), 1, y, 1, 1),
                )
            )

    def ring_y(self, k, z0, nz, part, right, cond):
        z, y = self.z, self.y
        if right:
            o, got, to = wrap(y - (k - 1)), wrap(y - k), wrap(y + 1)
        else:
            o, got, to = lax.rem(y + k - 1, N), lax.rem(y + k, N), wrap(y - 1)
        return self.transfer(
            cond,
            self.view(z0, nz, o, 1, part),
            self.view(z0, nz, o, 1, part),
            self.dev(z, to),
            cond,
            self.view(z0, nz, got, 1, part),
        )

    def hop_a(self, right, sub, k, depth):
        z, y = self.z, self.y
        y0, ny = (sub * 4, 4)
        if right:
            o, got, to = wrap(z - (k - 1)), wrap(z - k), wrap(z + 1)
            cs = both(z - (k - 1) >= 0, z + 1 < self.rows) if self.causal else True
            cr = both(self.live, z - k >= 0) if self.causal else True
        else:
            o, got, to = wrap(z + k - 1), lax.rem(z + k, N), wrap(z - 1)
            cs = o < depth if self.causal else True
            cr = got < depth if self.causal else True
        return self.transfer(
            cs,
            self.view(o, 1, y0, ny, 0),
            self.view(o, 1, y0, ny, 0),
            self.dev(to, y),
            cr,
            self.view(got, 1, y0, ny, 0),
        )

    def hop_b(self, right, sub, k):
        z0, nz = self.subs_b[sub]
        cond = self.live
        if self.causal and z0 > 0:
            cond = both(cond, self.z >= z0)
        return self.ring_y(k, z0, nz, 1, right, cond)

    def depth_a(self, right, sub):
        if self.rows < N:
            return self.rows - 1 if right else 0
        return 4 if right == (sub == 0) else 3

    def depth_b(self, right, sub):
        return 4 if right == ((sub % 2 == 0) != self.tie) else 3

    def hop(self, k):
        steps = []
        order = [("a", 0), ("b", 0), ("b", 1), ("a", 1)] + [("b", i) for i in range(2, 5)]
        begun = set()
        for ring, s in order:
            if s >= (2 if ring == "a" else len(self.subs_b)) or not self.parts[ring == "b"]:
                continue
            if k == 1 and ring not in begun:
                begun.add(ring)
                steps.append(lambda ring=ring: self.begin(ring))
            for r in (True, False):
                steps.append(lambda ring=ring, s=s, r=r: self.lane(ring, s, r, k))
        return steps

    def begin(self, ring):
        for t in self.a1 if ring == "a" else self.b1:
            self.take(t)

    def lane(self, ring, s, r, k):
        depth = self.depth_a(r, s) if ring == "a" else self.depth_b(r, s)
        got = None
        if 1 < k <= depth + 1:
            got = self.flight[ring, r, s]
            self.take(got)
        if k <= depth:
            self.flight[ring, r, s] = (
                self.hop_a(r, s, k, depth) if ring == "a" else self.hop_b(r, s, k)
            )
        if got is not None:
            self.mirror(got[1], got[2])
        if k == 1 and r:
            if ring == "a":
                self.mirror(self.live, self.view(self.z, 1, s * 4, 4, 0))
            else:
                z0, nz = self.subs_b[s]
                cond = both(self.live, self.z >= z0) if z0 and self.causal else self.live
                self.mirror(cond, self.view(z0, nz, self.y, 1, 1))

    def last(self):
        for i, send, recv, ref in self.pair_waits:
            when(recv, lambda: self.c.arrived(i, ref, self.pair))
            when(send, lambda: self.c.left(i, ref, self.pair))
        for i, cond, ref, device in self.waits:
            when(cond, lambda: self.c.left(i, ref, device))


def spread_partners(dp, tp):
    return [{"dp": lax.rem(dp + e // 2, 4), "tp": lax.rem(tp + e % 2, 2)} for e in range(1, 8)]


def entry_kernel(
    x_ref,
    w_ref,
    o_ref,
    ints_ref,
    wg_ref,
    qkv_ref,
    gate_ref,
    wo_ref,
    gint_ref,
    tok_ref,
    wall_ref,
    wcat_ref,
    wg_buf,
    send_sems,
    recv_sems,
    int_sems,
    local_sem,
    gate_sem,
):
    z, y = place()
    dp, tp = lax.axis_index("dp"), lax.axis_index("tp")
    pair = {"tp": 1 - tp}
    owner = dp // 2 == tp
    mine = x_ref.at[pl.ds(pl.multiple_of(tp * HALF, HALF), HALF)]
    local = pltpu.make_async_copy(mine, tok_ref.at[dp], local_sem)
    local.start()
    gate_copy = pltpu.make_async_copy(wg_ref, wg_buf, gate_sem)
    gate_copy.start()
    wo_ref[tp, z, y] = o_ref[...]

    @pl.when(owner)
    def _():
        wall_ref[z, y] = w_ref[...]

    barrier(plane_partners(z, y) + spread_partners(dp, tp))
    c = Copies(send_sems, recv_sems)

    left, right = lax.rem(dp + 3, 4), lax.rem(dp + 1, 4)
    part = HALF // 2
    first = {}
    for way, to, subs in (("r", right, (0, 1)), ("l", left, (1, 0))):
        for sub in subs:
            i = c.slot()
            src = x_ref.at[pl.ds(pl.multiple_of(tp * HALF + sub * part, part), part)]
            c.send(i, src, tok_ref.at[dp, pl.ds(sub * part, part)], {"dp": to})
            first[way, sub] = (i, src, to)

    def int_copy(gl, h):
        return pltpu.make_async_remote_copy(
            src_ref=ints_ref.at[gl, h],
            dst_ref=gint_ref.at[dp],
            send_sem=int_sems.at[gl * 2 + h],
            recv_sem=int_sems.at[4 + dp],
            device_id={"dp": 2 * tp + gl, "tp": jnp.int32(h)},
            device_id_type=MESH,
        )

    def is_own(gl, h):
        return jnp.logical_and(2 * tp + gl == dp, tp == h)

    for gl in range(2):
        for h in range(2):

            def go(gl=gl, h=h):
                int_copy(gl, h).start()

            def keep(gl=gl, h=h):
                gint_ref[dp] = ints_ref[gl, h]

            pl.when(jnp.logical_not(is_own(gl, h)))(go)
            pl.when(is_own(gl, h))(keep)

    jobs = []
    for src_ref, out_ref, only in ((o_ref, wo_ref.at[tp], True), (w_ref, wall_ref, owner)):
        half = src_ref.shape[0] // 2

        def src(part, src_ref=src_ref, half=half):
            return src_ref.at[pl.ds(part * half, half)]

        def view(z0, nz, y0, ny, part, out_ref=out_ref, half=half):
            zi = z0 if nz == 1 else pl.ds(z0, nz)
            yi = y0 if ny == 1 else pl.ds(y0, ny)
            return out_ref.at[zi, yi, pl.ds(part * half, half)]

        jobs.append(Gather(c, src, view, N, False, pair, only=only))
    for g in jobs:
        g.first()
    second = []

    def onward(way, sub, frm, to):
        i = first[way, sub][0]
        ref = tok_ref.at[frm, pl.ds(sub * part, part)]
        c.arrived(i, ref, {"dp": to})
        i2 = c.slot()
        c.send(i2, ref, ref, {"dp": to})
        second.append((i2, ref, sub, to))

    for k in range(1, 6):
        for g in jobs:
            for step in g.hop(k):
                step()
        if k == 2:
            onward("r", 0, left, right)
            onward("l", 1, right, left)
    assert c.used <= send_sems.shape[0], c.used
    for g in jobs:
        g.last()

    frm_col = lax.broadcasted_iota(jnp.int32, (2 * HEADS, 128), 0)
    to_col = lax.broadcasted_iota(jnp.int32, (2 * HEADS, 128), 1)
    wanted = (to_col >> 2) * HEADS + dp * PER + (to_col & 3)
    chosen = jnp.logical_and(frm_col == wanted, to_col < 8)
    gate_copy.wait()
    width = wall_ref.shape[3]
    wcat_ref[:, pl.ds(0, width)] = wall_ref[...].reshape(wcat_ref.shape[0], width)
    wcat_ref[:, pl.ds(width, 128)] = lax.dot_general(
        wg_buf[...],
        jnp.where(chosen, 1.0, 0.0).astype(jnp.bfloat16),
        (((0,), (0,)), ((), ())),
        preferred_element_type=jnp.float32,
    ).astype(jnp.bfloat16)

    def project(q):
        got = jnp.dot(tok_ref[q], wcat_ref[...], preferred_element_type=jnp.float32)
        qkv_ref[q] = got[:, :width].astype(jnp.bfloat16)
        gate_ref[q] = lax.logistic(got[:, width : width + 16])

    local.wait()
    project(dp)
    for q in range(4):

        def take(q=q):
            ref = gint_ref.at[q]
            pltpu.make_async_remote_copy(
                src_ref=ref,
                dst_ref=ref,
                send_sem=int_sems.at[0],
                recv_sem=int_sems.at[4 + q],
                device_id={"dp": jnp.int32(q), "tp": tp},
                device_id_type=MESH,
            ).wait_recv()

        pl.when(jnp.logical_not(jnp.logical_and(q == dp, owner)))(take)
    for gl in range(2):
        for h in range(2):
            pl.when(jnp.logical_not(is_own(gl, h)))(lambda gl=gl, h=h: int_copy(gl, h).wait_send())
    for way, sub, frm, to in (("r", 1, left, right), ("l", 0, right, left)):
        c.arrived(first[way, sub][0], tok_ref.at[frm, pl.ds(sub * part, part)], {"dp": to})
        project(frm)
    far = lax.rem(dp + 2, 4)
    for i2, ref, sub, to in second:
        c.arrived(i2, tok_ref.at[far, pl.ds(sub * part, part)], {"dp": to})
    project(far)
    for i, src, to in first.values():
        c.left(i, src, {"dp": to})
    for i2, ref, sub, to in second:
        c.left(i2, ref, {"dp": to})


def entry(x, w, o, ints, wg):
    vm = pl.BlockSpec(memory_space=VMEM)
    hbm = pl.BlockSpec(memory_space=HBM)
    return pl.pallas_call(
        entry_kernel,
        out_shape=[
            jax.ShapeDtypeStruct((4, HALF, w.shape[1]), x.dtype),
            jax.ShapeDtypeStruct((4, HALF, 16), jnp.float32),
            jax.ShapeDtypeStruct((2, N, N) + o.shape, o.dtype),
            jax.ShapeDtypeStruct((4,) + ints.shape[2:], ints.dtype),
        ],
        in_specs=[hbm, vm, vm, vm, hbm],
        out_specs=[vm] * 4,
        scratch_shapes=[
            pltpu.VMEM((4, HALF, x.shape[1]), x.dtype),
            pltpu.VMEM((N, N) + w.shape, w.dtype),
            pltpu.VMEM((x.shape[1], w.shape[1] + 128), w.dtype),
            pltpu.VMEM(wg.shape, wg.dtype),
            pltpu.SemaphoreType.DMA((192,)),
            pltpu.SemaphoreType.DMA((192,)),
            pltpu.SemaphoreType.DMA((8,)),
            pltpu.SemaphoreType.DMA,
            pltpu.SemaphoreType.DMA,
        ],
        compiler_params=pltpu.CompilerParams(
            collective_id=0, has_side_effects=True, vmem_limit_bytes=60 << 20
        ),
        cost_estimate=pl.CostEstimate(
            flops=30_000_000_000, bytes_accessed=8 << 20, transcendentals=0
        ),
        name="entry",
    )(x, w, o, ints, wg)


def bases(spans):
    return [sum(spans[:r]) for r in range(4)]


def kv_kernel(spans, order_ref, got_ref, pairs_ref, out_ref, own, send_sems, recv_sems):
    z, y = place()
    tp = lax.axis_index("tp")
    pair = {"tp": 1 - tp}
    base = bases(spans)
    for r, rows in enumerate(spans):

        def fill(r=r):
            seq = order_ref[r]
            piece = got_ref[seq, :, pl.ds(PER * HEAD, 2 * HEAD)]
            pairs = pairs_ref[seq]
            for ref in (own.at[r], out_ref.at[tp, base[r] + z, y]):
                ref[pl.ds(0, HALF)] = piece
                ref[pl.ds(HALF, ROWS - HALF)] = pairs

        when(True if rows == N else z < rows, fill)
    barrier(plane_partners(z, y) + [pair])
    c = Copies(send_sems, recv_sems)
    jobs = []
    for r, rows in enumerate(spans):

        split = SPLIT if r == 0 else 0

        def part_rows(part, split=split):
            return pl.ds(0, split) if part == 0 else pl.ds(split, ROWS - split)

        def src(part, r=r, part_rows=part_rows):
            return own.at[r, part_rows(part)]

        def view(z0, nz, y0, ny, part, r=r, part_rows=part_rows):
            zi = base[r] + z0 if nz == 1 else pl.ds(base[r] + z0, nz)
            yi = y0 if ny == 1 else pl.ds(y0, ny)
            return out_ref.at[tp, zi, yi, part_rows(part)]

        jobs.append(Gather(c, src, view, rows, True, pair, (r == 0, True), r % 2 == 1))
    for g in jobs:
        g.first()
    for k in range(1, 6):
        for g in jobs:
            for step in g.hop(k):
                step()
    assert c.used <= send_sems.shape[0], c.used
    for g in jobs:
        g.last()


def gather_kv(order, got, pairs, spans, number, limit):
    vm = pl.BlockSpec(memory_space=VMEM)
    return pl.pallas_call(
        functools.partial(kv_kernel, spans),
        out_shape=jax.ShapeDtypeStruct((2, sum(spans), N, ROWS, 2 * HEAD), got.dtype),
        in_specs=[pl.BlockSpec(memory_space=SMEM), vm, vm],
        out_specs=vm,
        scratch_shapes=[
            pltpu.VMEM((4, ROWS, 2 * HEAD), jnp.bfloat16),
            pltpu.SemaphoreType.DMA((limit,)),
            pltpu.SemaphoreType.DMA((limit,)),
        ],
        compiler_params=pltpu.CompilerParams(
            collective_id=number,
            has_side_effects=True,
            vmem_limit_bytes=(24 if sum(spans) < 20 else 40) << 20,
        ),
        cost_estimate=pl.CostEstimate(
            flops=30_000_000_000, bytes_accessed=8 << 20, transcendentals=0
        ),
        name="gather_kv",
    )(order, got, pairs)


def attend_kernel(
    spans, order_ref, ints_ref, main_ref, gate_ref, kv_ref, block_ref, out_ref, buf, comp
):
    kv, tp = lax.axis_index("kv"), lax.axis_index("tp")
    start = kv * (2 * HALF) + tp * HALF
    base = bases(spans)
    lane = lax.broadcasted_iota(jnp.int32, (BLK, 128), 1)
    row_in = lax.rem(lax.broadcasted_iota(jnp.int32, (PER * BLK, 1), 0), BLK)
    comp[...] = jnp.zeros_like(comp)
    to_row = lax.broadcasted_iota(jnp.int32, (48, 256), 0)
    from_row = lax.broadcasted_iota(jnp.int32, (48, 256), 1)
    piece = (to_row * 21846) >> 16
    pick_rows = jnp.where(from_row == piece * 16 + (to_row - piece * 3), 1.0, 0.0).astype(jnp.bfloat16)
    block_ends = block_ref[...] * BLK + (BLK - 1)

    def step(n, carry):
        r = (n * 21846) >> 16
        j = n - r * 3
        seq = order_ref[r]
        rows = pl.ds(pl.multiple_of(j * BLK, BLK), BLK)
        live = start < ints_ref[seq, 7, 0]
        first = jnp.int32(base[0])
        for q in range(1, 4):
            first = jnp.where(r == q, base[q], first)

        @pl.when(jnp.logical_and(live, j == 0))
        def _():
            def pack(zs):
                for z in zs:
                    at = jnp.minimum(first + z, sum(spans) - 1)
                    tile = kv_ref[:, at, :, pl.ds(HALF, 16), :].reshape(256, 128)
                    got = jnp.dot(pick_rows, tile, preferred_element_type=jnp.float32)
                    got = jnp.where(z <= kv // N, got, 0.0)
                    comp[pl.ds(z * 48, 48), :] = got.astype(jnp.bfloat16)

            pack((0, 1))
            pl.when(kv >= 2 * N)(lambda: pack((2, 3)))
            pl.when(kv >= 4 * N)(lambda: pack((4, 5, 6, 7)))

        @pl.when(jnp.logical_not(live))
        def _():
            out_ref[seq, rows] = jnp.zeros((BLK, PER * HEAD), jnp.bfloat16)

        @pl.when(live)
        def _():
            def fetch(p, count):
                b = ints_ref[seq, j, p]

                @pl.when(b >= 0)
                def _():
                    span = (b * 10923) >> 16
                    at = b - span * 6
                    t = jnp.where(at >= 3, 1, 0)
                    row = (at - t * 3) * BLK
                    buf[pl.ds(pl.multiple_of(count * BLK, BLK), BLK), :] = kv_ref[
                        t,
                        first + (span >> 3),
                        span & 7,
                        pl.ds(pl.multiple_of(row, BLK), BLK),
                        :,
                    ]

                return count + jnp.where(b >= 0, 1, 0)

            count = ints_ref[seq, j, PICKS]

            @pl.when(count > 0)
            def _():
                lax.fori_loop(0, PICKS, fetch, jnp.int32(0), unroll=True)

            parts = []
            for h in range(PER):
                two = main_ref[seq, rows, pl.ds((h // 2) * 128, 128)].astype(jnp.float32) * 0.125
                if h % 2:
                    two = pltpu.roll(two, 64, 1)
                parts.append(jnp.where(lane < HEAD, two, 0.0).astype(jnp.bfloat16))
            q = jnp.concatenate(parts, axis=0)

            def score(keys):
                return lax.dot_general(
                    q, keys, (((1,), (1,)), ((), ())), preferred_element_type=jnp.float32
                )

            spot = start + j * BLK + row_in
            own = main_ref[seq, rows, pl.ds(PER * HEAD, 128)]
            ks = lax.broadcasted_iota(jnp.int32, (1, BLK), 1)

            def run(most, far_too):
                keys = comp[pl.ds(0, most), :]
                cs = jnp.where(block_ends[:, :most] <= spot, score(keys), MASKED)
                ctop = jnp.max(cs, axis=-1, keepdims=True)
                cw = jnp.exp(cs - ctop)
                cn = jnp.maximum(jnp.sum(cw, axis=-1, keepdims=True), 1.0)
                cp = (cw * jnp.where(spot >= BLK - 1, 1.0 / cn, 0.0)).astype(jnp.bfloat16)
                co = jnp.dot(cp, keys, preferred_element_type=jnp.float32)

                os = jnp.where(ks <= row_in, score(own), MASKED)
                top = jnp.max(os, axis=-1, keepdims=True)
                if far_too:
                    far = buf[...]
                    spots = lax.broadcasted_iota(jnp.int32, (1, PICKS * BLK), 1)
                    fs = jnp.where(spots < count * BLK, score(far), MASKED)
                    top = jnp.maximum(top, jnp.max(fs, axis=-1, keepdims=True))
                ow = jnp.exp(os - top)
                total = jnp.sum(ow, axis=-1, keepdims=True)
                if far_too:
                    fw = jnp.exp(fs - top)
                    total = total + jnp.sum(fw, axis=-1, keepdims=True)
                inv = 1.0 / total
                so = jnp.dot((ow * inv).astype(jnp.bfloat16), own, preferred_element_type=jnp.float32)
                if far_too:
                    so = so + jnp.dot(
                        (fw * inv).astype(jnp.bfloat16), far, preferred_element_type=jnp.float32
                    )
                mixed = []
                g = gate_ref[seq, rows]
                for h in range(PER):
                    at = slice(h * BLK, (h + 1) * BLK)
                    mixed.append(g[:, h : h + 1] * co[at] + g[:, 4 + h : 5 + h] * so[at])
                for h in range(2):
                    pair = jnp.where(
                        lane < HEAD, pltpu.roll(mixed[2 * h], 64, 1), mixed[2 * h + 1]
                    )
                    out_ref[seq, rows, pl.ds(h * 128, 128)] = pair.astype(jnp.bfloat16)

            low, some = kv < 2 * N, count > 0
            for cond_low, most in ((low, 128), (jnp.logical_not(low), 384)):
                for cond_far, far_too in ((some, True), (jnp.logical_not(some), False)):
                    pl.when(jnp.logical_and(cond_low, cond_far))(
                        functools.partial(run, most, far_too)
                    )

        return carry

    buf[...] = jnp.zeros_like(buf)
    lax.fori_loop(0, 12, step, 0)


def attend(spans, order, gint, got, gates, gathered):
    vm = pl.BlockSpec(memory_space=VMEM)
    sm = pl.BlockSpec(memory_space=SMEM)
    c = jnp.arange(384, dtype=jnp.int32)
    z, t, y, j = c // 48, c % 48 // 24, c % 24 // 3, c % 3
    blocks = ((z * N + y) * 6 + t * 3 + j)[None]
    return pl.pallas_call(
        functools.partial(attend_kernel, spans),
        out_shape=jax.ShapeDtypeStruct((4, HALF, PER * HEAD), jnp.bfloat16),
        in_specs=[sm, sm, vm, vm, vm, vm],
        out_specs=vm,
        scratch_shapes=[
            pltpu.VMEM((PICKS * BLK, 2 * HEAD), jnp.bfloat16),
            pltpu.VMEM((384, 2 * HEAD), jnp.bfloat16),
        ],
        compiler_params=pltpu.CompilerParams(vmem_limit_bytes=(24 if sum(spans) < 20 else 48) << 20),
        name="attend",
    )(order, gint, got, gates, gathered, blocks)


def finish_kernel(len_ref, att_ref, wo_ref, out_ref, back, send_sems, recv_sems):
    dp, kv, tp = lax.axis_index("dp"), lax.axis_index("kv"), lax.axis_index("tp")
    barrier([{"dp": lax.rem(dp + d, 4)} for d in range(1, 4)])

    def copy(d):
        to = lax.rem(dp + d, 4)
        return pltpu.make_async_remote_copy(
            src_ref=att_ref.at[to],
            dst_ref=back.at[dp],
            send_sem=send_sems.at[d],
            recv_sem=recv_sems.at[d],
            device_id={"dp": to},
            device_id_type=MESH,
        )

    for d in (2, 1, 3):
        copy(d).start()
    back[dp] = att_ref[dp]

    def arrived(frm):
        d = lax.rem(dp + 4 - frm, 4)
        pltpu.make_async_remote_copy(
            src_ref=back.at[frm],
            dst_ref=back.at[frm],
            send_sem=send_sems.at[d],
            recv_sem=recv_sems.at[d],
            device_id={"dp": frm},
            device_id_type=MESH,
        ).wait_recv()

    spot = kv * (2 * HALF) + tp * HALF + lax.broadcasted_iota(jnp.int32, (HALF, 1), 0)
    alive = spot < len_ref[0]

    def tiles(t, last):
        cols = jnp.concatenate([back[2 * t], back[2 * t + 1]], axis=1)

        def tile(z, carry):
            w = wo_ref[t, z].reshape(256, 512)
            part = lax.dot_general(
                cols, w, (((1,), (1,)), ((), ())), preferred_element_type=jnp.float32
            ).astype(jnp.bfloat16)
            at = pl.ds(pl.multiple_of(z * 256, 256), 256)
            if last:
                both_sets = out_ref[:, at].astype(jnp.float32) + part.astype(jnp.float32)
                part = jnp.where(alive, both_sets, 0.0).astype(jnp.bfloat16)
            out_ref[:, at] = part
            return carry

        lax.fori_loop(0, N, tile, 0, unroll=2)

    near = dp // 2
    arrived(4 * near + 1 - dp)
    tiles(near, False)
    arrived(2 - 2 * near)
    arrived(3 - 2 * near)
    tiles(1 - near, True)
    for d in (1, 2, 3):
        copy(d).wait_send()


def finish(length, att, wo, number):
    vm = pl.BlockSpec(memory_space=VMEM)
    return pl.pallas_call(
        finish_kernel,
        out_shape=jax.ShapeDtypeStruct((HALF, 2048), jnp.bfloat16),
        in_specs=[pl.BlockSpec(memory_space=SMEM), vm, vm],
        out_specs=vm,
        scratch_shapes=[
            pltpu.VMEM((4, HALF, PER * HEAD), jnp.bfloat16),
            pltpu.SemaphoreType.DMA((4,)),
            pltpu.SemaphoreType.DMA((4,)),
        ],
        compiler_params=pltpu.CompilerParams(
            collective_id=number, has_side_effects=True, vmem_limit_bytes=24 << 20
        ),
        name="finish",
    )(length, att, wo)


def body(
    tokens, seq_lengths, block_picks, w_query, w_key, w_value, w_gate, w_ckey, w_cvalue, w_out
):
    x = tokens[0]
    dp = lax.axis_index("dp")
    low = lax.rem(dp, 2) == 0
    piece = jnp.where(
        low,
        jnp.concatenate([w_query[:, :256], w_key[:, :64], w_value[:, :64]], axis=1),
        jnp.concatenate([w_query[:, 256:], w_key[:, 64:], w_value[:, 64:]], axis=1),
    )
    picks = block_picks[0].transpose(1, 0, 2).reshape(2, 2, 3, PICKS)
    valid = jnp.sum((picks >= 0).astype(jnp.int32), axis=3, keepdims=True)
    ints = jnp.pad(picks, ((0, 0), (0, 0), (0, 5), (0, 112)))
    valid = jnp.pad(valid, ((0, 0), (0, 0), (0, 5), (0, 0)))
    row = lax.broadcasted_iota(jnp.int32, ints.shape, 2)
    col = lax.broadcasted_iota(jnp.int32, ints.shape, 3)
    ints = jnp.where(row == 7, seq_lengths[0], jnp.where(col == PICKS, valid, ints))
    got, gates, wo, gint = entry(x, piece, w_out.T, ints, w_gate.T)

    qkv = got.reshape(4 * HALF, 384)
    flat = qkv.reshape(12, BLK, 384)
    ck = jnp.dot(
        flat[..., 256:320].reshape(12, BLK * HEAD), w_ckey, preferred_element_type=jnp.float32
    )
    cv = jnp.dot(
        flat[..., 320:].reshape(12, BLK * HEAD), w_cvalue, preferred_element_type=jnp.float32
    )
    pairs = jnp.concatenate([ck, cv], axis=1).astype(jnp.bfloat16).reshape(4, 3, 128)
    pairs = jnp.pad(pairs, ((0, 0), (0, 13), (0, 0)))
    lens = gint[:, 7, 0]
    ids = jnp.arange(4, dtype=jnp.int32)
    ahead = (lens[None, :] > lens[:, None]) | (
        (lens[None, :] == lens[:, None]) & (ids[None, :] < ids[:, None])
    )
    rank = jnp.sum(ahead.astype(jnp.int32), axis=1)
    order = jnp.sum(jnp.where(rank[None, :] == ids[:, None], ids[None, :], 0), axis=1)
    ranked = jnp.sum(
        jnp.where(rank[None, :] == ids[:, None], lens[None, :], 0), axis=1
    )

    def run(spans, number, limit):
        gathered = gather_kv(order, got, pairs, spans, number, limit)
        att = attend(spans, order, gint, got, gates, gathered)
        return finish(seq_lengths, att, wo, number + 1)

    span = N * 384
    small = (ranked[1] <= 3 * span) & (ranked[2] <= 2 * span) & (ranked[3] <= span)
    out = lax.cond(
        small, lambda: run((8, 3, 2, 1), 2, 448), lambda: run((8, 8, 8, 8), 4, 600)
    )
    return out[None]


def solution(mesh):
    return jax.shard_map(
        body,
        mesh=mesh,
        in_specs=(
            P("dp", "kv", None),
            P("dp"),
            P("dp", "kv", "tp", None),
            P("kv", "tp"),
            P("kv", "tp"),
            P("kv", "tp"),
            P(),
            P(),
            P(),
            P("tp", "kv"),
        ),
        out_specs=P("dp", ("kv", "tp"), None),
        check_vma=False,
    )
```
